32 devices in a mesh: sp: 4 (over z), dp: 8 (over y, x, core).
Axes of the slice: x: 2, y: 2, z: 4, core: 2. Of those that a mesh axis runs over, the one named last changes fastest.
Arguments:
- queries: bfloat16 [8, 768, 1024], P('dp', 'sp'), may hold values from -6 to 6
- keys: bfloat16 [8, 768, 256], P('dp', 'sp'), may hold values from -6 to 6
- values: bfloat16 [8, 768, 256], P('dp', 'sp'), may hold values from -6 to 6
- query_gain: float32 [64], replicated, may hold values from 0.15 to 7
- key_gain: float32 [64], replicated, may hold values from 0.15 to 7
- out_weight: bfloat16 [1024, 2048], P(None, 'dp'), may hold values from -0.1875 to 0.1875
- out_gain: float32 [2048], replicated, may hold values from 0.1 to 1.9
Outputs:
- output: bfloat16 [8, 768, 2048], P('dp', 'sp')
The draws below stay inside these ranges and needn't reach their ends.
All inputs are finite; a program needn't handle non-finite values.
Results may differ from the reference program's by a relative error of at most 0.0035.
The reference program's roundings to bfloat16 on the way (of `attn_weights` and `attended`) count: a program that leaves them out, or rounds other values in their place, can miss the bound.
Values may be sent and summed in bfloat16 or wider, within the bound.
A program may use at most 64 MiB of HBM per device.

```python
import jax
import jax.numpy as jnp
from jax import lax

D = 2048
QH = 16
KVH = 4
HEAD = 64
GRID_W = 64
SEQ = 768
N_DP = 8


def query_key_pair(key):
    base_key = jax.random.fold_in(key, 11)
    key_a, key_b = jax.random.split(base_key, 2)
    key_draw = jax.random.normal(key_a, (N_DP, SEQ, KVH, HEAD), jnp.float32)
    query_draw = jax.random.normal(key_b, (N_DP, SEQ, QH, HEAD), jnp.float32)
    query_draw = jnp.clip(query_draw, -6.0, 6.0).reshape(N_DP, SEQ, QH * HEAD)
    key_draw = jnp.clip(key_draw, -6.0, 6.0).reshape(N_DP, SEQ, KVH * HEAD)
    return (query_draw, key_draw)


def gain_draw(key, salt):
    spread = 1.0 + 0.18 * jnp.clip(jax.random.normal(jax.random.fold_in(key, salt), (HEAD,), jnp.float32), -4.5, 4.5)
    return spread


def draw_queries(key, part):
    return query_key_pair(key)[0].astype(jnp.bfloat16)


def draw_keys(key, part):
    return query_key_pair(key)[1].astype(jnp.bfloat16)


def draw_query_gain(key, part):
    return gain_draw(key, 21)


def draw_key_gain(key, part):
    return gain_draw(key, 22)


def levels(stream_key, dims, cuts, least, largest):
    def one(dim, parts):
        steps = jax.random.uniform(jax.random.fold_in(jax.random.fold_in(stream_key, 6), dim), (parts,), jnp.float32, least / len(cuts), largest / len(cuts))
        return jnp.repeat(jnp.exp(steps), dims[dim] // parts).reshape((-1,) + (1,) * (len(dims) - dim - 1))

    level = one(*cuts[0])
    for cut in cuts[1:]:
        level = level * one(*cut)
    return level


def bell_draw(own_key, extent, scale, most, cuts=(), held_as=jnp.bfloat16):
    factor_of = levels(own_key, extent, cuts, -0.22, 0.18) if cuts else 1.0
    values = jax.random.normal(own_key, extent, jnp.float32) * scale * factor_of
    return jnp.minimum(jnp.maximum(values, -most), most).astype(held_as)


def setup_inputs(seed: int = 0) -> dict:
    streams_of = jax.random.split(jax.random.key(seed), 8)
    return {
        "queries": draw_queries(jax.random.fold_in(streams_of[7], 71), 0),
        "keys": draw_keys(jax.random.fold_in(streams_of[7], 71), 0),
        "values": bell_draw(streams_of[2], (N_DP, SEQ, KVH * HEAD), 1.0, 6.0, ((0, 8), (1, 4))),
        "query_gain": draw_query_gain(jax.random.fold_in(streams_of[7], 71), 0),
        "key_gain": draw_key_gain(jax.random.fold_in(streams_of[7], 71), 0),
        "out_weight": bell_draw(streams_of[5], (QH * HEAD, D), (QH * HEAD) ** -0.5, 0.1875, ((1, 8),)),
        "out_gain": jnp.clip(1.0 + 0.18 * jax.random.normal(streams_of[6], (D,), jnp.float32), 0.1, 1.9),
    }


EPSILON = 1e-06
ROTARY_BASE = 10000.0

def rotate(vectors, positions, width):
    half_width = width // 2
    frequency = ROTARY_BASE ** (-jnp.arange(0, width, 2, dtype=jnp.float32) / width)
    angles = positions.astype(jnp.float32)[:, None] * frequency[None, :]
    cosines = jnp.cos(angles)[:, None, :]
    sine_table = jnp.sin(angles)[:, None, :]
    first_half = vectors[..., :half_width]
    second_half = vectors[..., half_width:]
    return jnp.concatenate([first_half * cosines - second_half * sine_table, second_half * cosines + first_half * sine_table], axis=-1)

def prepare(vectors, gain_vector, grid_row, grid_col):
    vectors = vectors.astype(jnp.float32)
    vectors = vectors * lax.rsqrt(lax.optimization_barrier(jnp.mean(vectors * vectors, axis=-1, keepdims=True)) + EPSILON) * gain_vector
    half_width = HEAD // 2
    turned = jnp.concatenate([rotate(vectors[..., :half_width], grid_row, half_width), rotate(vectors[..., half_width:], grid_col, half_width)], axis=-1)
    return turned.astype(jnp.bfloat16)

def reference(queries, keys, values, query_gain, key_gain, out_weight, out_gain):
    positions = jnp.arange(SEQ, dtype=jnp.int32)
    grid_row = positions // GRID_W
    grid_col = positions % GRID_W
    group_size = QH // KVH
    score_scale = HEAD ** (-0.5)

    def one_sequence(operands):
        query_seq, key_seq, value_seq = operands
        query_rot = prepare(query_seq.reshape(SEQ, QH, HEAD), query_gain, grid_row, grid_col)
        key_rot = prepare(key_seq.reshape(SEQ, KVH, HEAD), key_gain, grid_row, grid_col)
        value_heads = value_seq.reshape(SEQ, KVH, HEAD)

        def one_head(head_index):
            query_head = lax.dynamic_index_in_dim(query_rot, head_index, 1, keepdims=False)
            key_head = lax.dynamic_index_in_dim(key_rot, head_index // group_size, 1, keepdims=False)
            value_head = lax.dynamic_index_in_dim(value_heads, head_index // group_size, 1, keepdims=False)
            scores = jnp.dot(query_head, key_head.T, preferred_element_type=jnp.float32) * score_scale
            row_max = lax.optimization_barrier(jnp.max(scores, axis=-1, keepdims=True))
            exponent = jnp.exp(scores - row_max)
            attn_weights = (exponent / lax.optimization_barrier(jnp.sum(exponent, axis=-1, keepdims=True))).astype(jnp.bfloat16)
            return jnp.dot(attn_weights, value_head, preferred_element_type=jnp.float32).astype(jnp.bfloat16)
        per_head = lax.map(one_head, jnp.arange(QH, dtype=jnp.int32))
        attended = per_head.transpose(1, 0, 2).reshape(SEQ, QH * HEAD)
        projected = jnp.dot(attended, out_weight, preferred_element_type=jnp.float32)
        projected = projected * lax.rsqrt(lax.optimization_barrier(jnp.mean(projected * projected, axis=-1, keepdims=True)) + EPSILON) * out_gain
        return projected.astype(jnp.bfloat16)
    return lax.map(one_sequence, (queries, keys, values))
```

```python
import functools

import jax
import jax.numpy as jnp
import numpy as np
from jax import lax
from jax.experimental import pallas as pl
from jax.experimental.pallas import tpu as pltpu
from jax.sharding import PartitionSpec as P

QH = 16
KVH = 4
HEAD = 64
GRID_W = 64
GROUP = QH // KVH
HALVES = 2
BLOCK = GROUP * HEAD
WIDTH = 128

TO_END = 64
TO_INNER = 160
CHUNKS = (256, 128, 128)
PIECES = 2 * (4 * len(CHUNKS) + 6) + 5


EPSILON = 1e-06
ROTARY_BASE = 10000.0

F32 = jnp.float32
BF16 = jnp.bfloat16


def rotate(vectors, positions, width):
    half_width = width // 2
    frequency = ROTARY_BASE ** (-jnp.arange(0, width, 2, dtype=jnp.float32) / width)
    angles = positions.astype(jnp.float32)[:, None] * frequency[None, :]
    cosines = jnp.cos(angles)[:, None, :]
    sine_table = jnp.sin(angles)[:, None, :]
    first_half = vectors[..., :half_width]
    second_half = vectors[..., half_width:]
    return jnp.concatenate(
        [
            first_half * cosines - second_half * sine_table,
            second_half * cosines + first_half * sine_table,
        ],
        axis=-1,
    )


def prepare(vectors, gain_vector, grid_row, grid_col):
    vectors = vectors.astype(jnp.float32)
    vectors = (
        vectors
        * lax.rsqrt(jnp.mean(vectors * vectors, axis=-1, keepdims=True) + EPSILON)
        * gain_vector
    )
    half_width = HEAD // 2
    turned = jnp.concatenate(
        [
            rotate(vectors[..., :half_width], grid_row, half_width),
            rotate(vectors[..., half_width:], grid_col, half_width),
        ],
        axis=-1,
    )
    return turned.astype(jnp.bfloat16)


def softmax_rows(scores):
    row_max = jnp.max(scores, axis=-1, keepdims=True)
    exponent = jnp.exp(scores - row_max)
    return exponent / jnp.sum(exponent, axis=-1, keepdims=True)


def per_device_general(queries, keys, values, query_gain, key_gain, out_weight, out_gain):
    sp_count = lax.axis_size("sp")
    tokens_here = queries.shape[1]
    seq_len = tokens_here * sp_count
    score_scale = HEAD ** (-0.5)
    offset = lax.axis_index("sp") * tokens_here
    positions = offset + jnp.arange(tokens_here, dtype=jnp.int32)
    grid_row = positions // GRID_W
    grid_col = positions % GRID_W
    query_rot = prepare(queries[0].reshape(tokens_here, QH, HEAD), query_gain, grid_row, grid_col)
    key_rot = prepare(keys[0].reshape(tokens_here, KVH, HEAD), key_gain, grid_row, grid_col)
    value_heads = values[0].reshape(tokens_here, KVH, HEAD)
    kv_pairs = jnp.concatenate([key_rot, value_heads], axis=2)
    all_pairs = lax.all_gather(
        kv_pairs.reshape(tokens_here, KVH * 2 * HEAD), "sp", axis=0, tiled=True
    )
    all_pairs = all_pairs.reshape(seq_len, KVH, 2, HEAD)
    key_all = all_pairs[:, :, 0].transpose(1, 0, 2)
    value_all = all_pairs[:, :, 1].transpose(1, 0, 2)
    query_groups = query_rot.reshape(tokens_here, KVH, QH // KVH, HEAD).transpose(1, 0, 2, 3)

    def attend_group(operands):
        query_group, key_head, value_head = operands
        scores = (
            jnp.einsum("qgd,kd->gqk", query_group, key_head, preferred_element_type=jnp.float32)
            * score_scale
        )
        attn_weights = softmax_rows(scores).astype(jnp.bfloat16)
        return jnp.einsum(
            "gqk,kd->qgd", attn_weights, value_head, preferred_element_type=jnp.float32
        ).astype(jnp.bfloat16)

    results = lax.map(attend_group, (query_groups, key_all, value_all))
    attended = results.transpose(1, 0, 2, 3).reshape(tokens_here, QH * HEAD)
    projected = jnp.dot(
        attended,
        lax.all_gather(out_weight, "dp", axis=1, tiled=True),
        preferred_element_type=jnp.float32,
    )
    normed = (
        projected
        * lax.rsqrt(jnp.mean(projected * projected, axis=-1, keepdims=True) + EPSILON)
        * out_gain
    )
    return normed.astype(jnp.bfloat16)[None]


def position_tables(seq_len):
    width = HEAD // 2
    frequency = np.float32(ROTARY_BASE) ** (
        -np.arange(0, width, 2, dtype=np.float32) / np.float32(width)
    )
    position = np.arange(seq_len)
    parts = []
    for coordinate in (position // GRID_W, position % GRID_W):
        angles = coordinate.astype(np.float32)[:, None] * frequency[None, :]
        parts += [angles, angles]
    angles = np.concatenate(parts * 2, axis=1).astype(np.float64)
    return np.stack([np.cos(angles), np.sin(angles)]).astype(np.float32)


def dot(a, b):
    return jnp.dot(a, b, preferred_element_type=F32)


def cross(a, b):
    return lax.dot_general(a, b, (((1,), (1,)), ((), ())), preferred_element_type=F32)


def kernel(
    sp, dp,
    q_ref, k_ref, v_ref, qg_ref, kg_ref, w_ref, og_ref, table_ref,
    out_ref,
    q_raw, k_all, v_all, tables, w_all, gains,
    swap_mat, ones_mat, q_t, v_turned,
    expo, peak, total, mixed, att, proj,
    local_sem, kv_send, kv_recv, w_send, w_recv,
):
    tokens = q_raw.shape[0]
    depth = w_ref.shape[0]
    half = depth // 2
    me = lax.axis_index("sp")
    here = lax.axis_index("dp")
    mate = here + 1 - 2 * (here % 2)
    flip_x = 2 - 4 * ((here // 2) % 2)
    flip_y = 4 - 8 * ((here // 4) % 2)
    dev_x = here + flip_x
    dev_y = here + flip_y
    dev_d = here + flip_x + flip_y

    barrier = pltpu.get_barrier_semaphore()
    has_left = me > 0
    has_right = me < sp - 1

    for other in (mate, dev_x, dev_y):
        pl.semaphore_signal(barrier, inc=1, device_id={"dp": other})

    @pl.when(has_left)
    def _():
        pl.semaphore_signal(barrier, inc=1, device_id={"sp": me - 1})

    @pl.when(has_right)
    def _():
        pl.semaphore_signal(barrier, inc=1, device_id={"sp": me + 1})

    locals_ = [
        pltpu.make_async_copy(k_ref, k_all.at[pl.ds(me * tokens, tokens)], local_sem.at[0]),
        pltpu.make_async_copy(v_ref, v_all.at[pl.ds(me * tokens, tokens)], local_sem.at[1]),
        pltpu.make_async_copy(w_ref, w_all.at[here], local_sem.at[2]),
        pltpu.make_async_copy(q_ref, q_raw, local_sem.at[3]),
        pltpu.make_async_copy(table_ref, tables, local_sem.at[4]),
    ]
    for copy in locals_:
        copy.start()
    for copy in locals_[:3]:
        copy.wait()

    pl.semaphore_wait(barrier, 3 + jnp.minimum(me, 1) + jnp.minimum(sp - 1 - me, 1))

    part = k_ref.shape[1] // HALVES

    stores = (k_all, v_all)

    def kv_copy(way, step, kind, side):
        block = me - step if way == 0 else me + step
        target = me + 1 if way == 0 else me - 1
        window = stores[kind].at[pl.ds(block * tokens, tokens), pl.ds(side * part, part)]
        return pltpu.make_async_remote_copy(
            src_ref=window,
            dst_ref=window,
            send_sem=kv_send.at[way, step, side, kind],
            recv_sem=kv_recv.at[way, step, side, kind],
            device_id={"sp": target},
        )

    def kv_sends(way, step):
        if way == 0:
            return jnp.logical_and(has_right, me - step >= 0)
        return jnp.logical_and(has_left, me + step < sp)

    def kv_start(way, step, kind, side):
        @pl.when(kv_sends(way, step))
        def _():
            kv_copy(way, step, kind, side).start()

    def kv_arrive(step, kind, side):
        for way in (0, 1):
            source = me - 1 - step if way == 0 else me + 1 + step
            arrives = source >= 0 if way == 0 else source < sp

            @pl.when(arrives)
            def _(way=way, source=source):
                window = stores[kind].at[
                    pl.ds(source * tokens, tokens), pl.ds(side * part, part)
                ]
                pltpu.make_async_remote_copy(
                    src_ref=window,
                    dst_ref=window,
                    send_sem=kv_send.at[way, step, side, kind],
                    recv_sem=kv_recv.at[way, step, side, kind],
                    device_id={"sp": me},
                ).wait_recv()

            if step + 1 < sp - 1:
                kv_start(way, step + 1, kind, side)

    for kind in (0, 1):
        for side in range(HALVES):
            for way in (1, 0):
                kv_start(way, 0, kind, side)

    odd = me % 2
    zmate = me + 1 - 2 * odd
    inner = (me + 1) // 2 % 2 == 1
    outer = jnp.logical_not(inner)
    shares = ((inner, 0, TO_END), (outer, half - TO_INNER, TO_INNER))
    mate_x, mate_y, mate_d = mate + flip_x, mate + flip_y, mate + flip_x + flip_y

    starts = [sum(CHUNKS[:j]) for j in range(len(CHUNKS))]
    pieces = {"own": (mate, 0, depth)}
    for j, (start, size) in enumerate(zip(starts, CHUNKS)):
        pieces["x", j] = (dev_x, half + start, size)
        pieces["y", j] = (dev_y, start, size)
        pieces["dx", j] = (dev_d, start, size)
        pieces["dy", j] = (dev_d, half + start, size)
    for name, shard, base in (("x", dev_x, 0), ("y", dev_y, half)):
        pieces[name, "middle"] = (shard, base + TO_END, half - TO_END - TO_INNER)
        for role, (_, start, size) in enumerate(shares):
            pieces[name, "share", role] = (shard, base + start, size)
    across = {"x": mate_x, "y": mate_y, "dx": mate_d, "dy": mate_d}
    for name in [name for name in pieces if name != "own"]:
        start, size = pieces[name][1:]
        pieces["mate", name] = (across[name[0]], start, size)
        if name[1] == "share":
            pieces["zed", name] = pieces[name]
    order = {name: i for i, name in enumerate(pieces)}
    sent = []

    def w_copy(name, shard, start, size, target):
        window = w_all.at[shard, pl.ds(start, size)]
        return pltpu.make_async_remote_copy(
            src_ref=window,
            dst_ref=window,
            send_sem=w_send.at[order[name]],
            recv_sem=w_recv.at[order[name]],
            device_id=target,
        )

    def w_give(name, shard, start, size, target):
        copy = w_copy(name, shard, start, size, target)
        copy.start()
        sent.append(copy)

    def w_own(name, target):
        w_give(name, here, *pieces[name][1:], {"dp": target})

    def w_wait(name):
        w_copy(name, *pieces[name], {"dp": mate}).wait_recv()

    def w_take(name):
        w_wait(name)
        piece = pieces[name]
        if name[1] in range(len(CHUNKS)):
            if name[0] == "x":
                w_give(("dy", name[1]), *piece, {"dp": dev_y})
            if name[0] == "y":
                w_give(("dx", name[1]), *piece, {"dp": dev_x})
        w_give(("mate", name), *piece, {"dp": mate})

    def w_share_own(name):
        for role, (chosen, _, _) in enumerate(shares):
            @pl.when(chosen)
            def _(key=(name, "share", role)):
                target = dev_x if name == "x" else dev_y
                w_copy(key, here, *pieces[key][1:], {"dp": target}).start()

    def w_share_near(name):
        for role, (chosen, _, _) in enumerate(shares):
            @pl.when(chosen)
            def _(key=(name, "share", role)):
                w_wait(key)
                w_copy(("zed", key), *pieces[key], {"sp": zmate}).start()
                w_copy(("mate", key), *pieces[key], {"dp": mate}).start()

    def w_share_far(name):
        for role in range(len(shares)):
            @pl.when(shares[1 - role][0])
            def _(key=(name, "share", role)):
                w_wait(("zed", key))
                w_copy(("mate", key), *pieces[key], {"dp": mate}).start()

    def w_share_sent(name):
        for role, (chosen, _, _) in enumerate(shares):
            key = (name, "share", role)
            w_copy(("mate", key), *pieces[key], {"dp": mate}).wait_send()

            @pl.when(chosen)
            def _(key=key):
                for form in (key, ("zed", key)):
                    w_copy(form, *pieces[key], {"dp": mate}).wait_send()

    for j in range(len(CHUNKS)):
        w_own(("x", j), dev_x)
        w_own(("y", j), dev_y)
    w_share_own("x")
    w_share_own("y")
    w_own(("x", "middle"), dev_x)
    w_own(("y", "middle"), dev_y)
    w_own("own", mate)

    row_id = lax.broadcasted_iota(jnp.int32, (BLOCK, BLOCK), 0)
    col_id = lax.broadcasted_iota(jnp.int32, (BLOCK, BLOCK), 1)
    quarter = HEAD // 4
    second = (col_id & (HEAD // 2 - 1)) >= quarter
    partner_col = jnp.where(second, col_id - quarter, col_id + quarter)
    hit = row_id == partner_col
    swap_mat[...] = jnp.where(hit, jnp.where(second, 1.0, -1.0), 0.0).astype(BF16)
    ones_mat[...] = jnp.where((row_id // HEAD) == (col_id // HEAD), 1.0, 0.0).astype(BF16)
    spread = jnp.where(
        row_id[:HEAD] == (col_id[:HEAD] & (HEAD - 1)), 1.0, 0.0
    ).astype(BF16)
    spread_swapped = jnp.where(
        row_id[:HEAD] == (partner_col[:HEAD] & (HEAD - 1)), 1.0, 0.0
    ).astype(BF16)
    for i, gain_ref in enumerate((qg_ref, kg_ref)):
        gain = jnp.broadcast_to(gain_ref[...], (16, HEAD))
        first = gain.astype(BF16)
        rest = gain - first.astype(F32)
        mid = rest.astype(BF16)
        low = (rest - mid.astype(F32)).astype(BF16)
        for j, matrix in enumerate((spread, spread_swapped)):
            gains[2 * i + j] = (dot(first, matrix) + dot(mid, matrix)) + dot(low, matrix)

    lane_head = lax.broadcasted_iota(jnp.int32, (1, BLOCK), 1) // HEAD
    masks = [jnp.where(lane_head == p, 1.0, 0.0).astype(BF16) for p in range(GROUP)]

    def turned(x, rows, which, scale):
        xf = x.astype(F32)
        square = xf * xf
        high = square.astype(BF16)
        low = (square - high.astype(F32)).astype(BF16)
        size = x.shape[1]
        ones = ones_mat[:size, :size]
        mean = (dot(high, ones) + dot(low, ones)) * (1.0 / HEAD)
        inverse = lax.rsqrt(mean + EPSILON) * scale
        swapped = dot(x, swap_mat[:size, :size])
        cosines = tables[0, rows, :]
        sines = tables[1, rows, :]
        if size > 2 * HEAD:
            cosines = jnp.concatenate([cosines, cosines], axis=1)
            sines = jnp.concatenate([sines, sines], axis=1)
        cosines = cosines * gains[2 * which, 0:1, :size]
        sines = sines * gains[2 * which + 1, 0:1, :size]
        return ((xf * cosines + swapped * sines) * inverse).astype(BF16)

    locals_[3].wait()
    locals_[4].wait()
    own_rows = pl.ds(pl.multiple_of(me * tokens, 64), tokens)
    for b in range(KVH):
        columns = slice(b * BLOCK, (b + 1) * BLOCK)
        query = turned(q_raw[:, columns], own_rows, 0, HEAD ** (-0.5))
        parts = [query[:WIDTH] * mask for mask in masks] + [query[WIDTH:] * mask for mask in masks]
        held = b % 2 * HEAD
        fold = jnp.where(row_id[:part] - held == (col_id[:part] & (HEAD - 1)), 1.0, 0.0)
        q_t[b] = cross(fold.astype(BF16), jnp.concatenate(parts, axis=0)).astype(BF16)

    eye = jnp.where(row_id == col_id, 1.0, 0.0).astype(BF16)
    far = 1 - me // 2
    blocks = [me, zmate, far + 1, 3 * far][:sp]
    spans = [pl.ds(pl.multiple_of(block * tokens, 64), tokens) for block in blocks]
    heads = KVH // HALVES
    rest = tokens - WIDTH
    final = sp - 1

    def score(turn, side):
        lanes = slice(side * part, (side + 1) * part)
        rows = spans[turn]
        key_side = turned(k_all[rows, lanes], rows, 1, 1.0)
        for b in range(side * heads, (side + 1) * heads):
            scores = dot(key_side, q_t[b])
            high = jnp.max(scores, axis=0, keepdims=True)
            if turn < final:
                weights = jnp.exp(scores - high)
                expo[turn, b] = weights
                peak[turn, b] = high
                total[turn, b] = jnp.sum(weights, axis=0, keepdims=True)
                continue
            for t in range(turn):
                high = jnp.maximum(high, peak[t, b])
            weights = jnp.exp(scores - high)
            norm = jnp.sum(weights, axis=0, keepdims=True)
            keeps = [jnp.exp(peak[t, b] - high) for t in range(turn)]
            for t in range(turn):
                norm = norm + total[t, b] * keeps[t]
            inverse = 1.0 / norm
            for t in range(turn):
                mixed[b, t * tokens : (t + 1) * tokens, :] = (
                    expo[t, b] * (keeps[t] * inverse)
                ).astype(BF16)
            mixed[b, turn * tokens :, :] = (weights * inverse).astype(BF16)

    def values(turn, side):
        lanes = slice(side * part, (side + 1) * part)
        pair = jnp.concatenate([v_all[spans[t], lanes] for t in (turn - 1, turn)], axis=0)
        width = slice((turn - 1) * tokens, (turn + 1) * tokens)
        v_turned[lanes, width] = cross(eye[:part, :part], pair).astype(BF16)

    def gather(side):
        for b in range(side * heads, (side + 1) * heads):
            value_rows = slice(b * HEAD, (b + 1) * HEAD)
            product = dot(v_turned[value_rows, :], mixed[b])
            for p in range(0, GROUP, 2):
                lanes = slice(b * BLOCK + p * HEAD, b * BLOCK + (p + 2) * HEAD)
                two = [product[:, i * WIDTH : (i + 1) * WIDTH] for i in (p, p + 1)]
                att[:WIDTH, lanes] = jnp.concatenate(two, axis=0).T.astype(BF16)
                start = GROUP * WIDTH + p * rest
                two = product[:, start : start + 2 * rest].T
                two = jnp.concatenate([two[:rest], two[rest:]], axis=1)
                att[WIDTH:, lanes] = two.astype(BF16)

    lots = len(CHUNKS)
    columns_each = w_ref.shape[1]
    late = CHUNKS[-1]
    tails = [half - late, depth - late]

    def columns_of(shard):
        return pl.ds(pl.multiple_of(shard * columns_each, columns_each), columns_each)

    def product(shard, start, size):
        rows = pl.ds(start, size)
        return dot(att[:, rows], w_all[shard, rows, :])

    def finish(shard, result, squares):
        proj[:, columns_of(shard)] = result
        return squares + jnp.sum(result * result, axis=1, keepdims=True)

    def project(shard, squares):
        return finish(shard, dot(att[...], w_all[shard]), squares)

    def begin(shard):
        proj[:, columns_of(shard)] = product(shard, 0, half - late) + product(
            shard, half, half - late
        )

    def end(shard, squares):
        result = proj[:, columns_of(shard)]
        for start in tails:
            result = result + product(shard, start, late)
        return finish(shard, result, squares)

    def take(*names):
        for name in names:
            w_take(("x", name))
            w_take(("y", name))

    def take_far(j):
        w_take(("dx", j))
        w_take(("dy", j))

    for side in range(HALVES):
        score(0, side)
    for step in range(sp - 1):
        last = step == sp - 2
        for side in range(HALVES):
            kv_arrive(step, 0, side)
            score(step + 1, side)
            if step == 0 and side == 0:
                take(0)
        for side in range(HALVES):
            kv_arrive(step, 1, side)
            if (step + 1) % 2:
                values(step + 1, side)
            if last:
                gather(side)
                if side == 0:
                    take_far(0)
            elif step == 0:
                take(side + 1)
        if step == max(sp - 3, 0):
            w_share_near("x")
            w_share_near("y")
            take("middle")

    squares = project(here, jnp.zeros((tokens, 1), F32))
    w_wait("own")
    squares = project(mate, squares)
    for j in range(1, lots - 1):
        take_far(j)
    for name in ("x", "y"):
        w_share_far(name)
    squares = project(dev_x, squares)
    squares = project(dev_y, squares)
    take_far(lots - 1)
    squares = project(dev_d, squares)
    for name, shard in (("x", mate_x), ("y", mate_y)):
        for piece in (*range(lots), "middle"):
            w_wait(("mate", (name, piece)))
        for role in range(len(shares)):
            w_wait(("mate", (name, "share", role)))
        squares = project(shard, squares)
    for j in range(lots - 1):
        w_wait(("mate", ("dx", j)))
        w_wait(("mate", ("dy", j)))
    begin(mate_d)
    w_wait(("mate", ("dx", lots - 1)))
    w_wait(("mate", ("dy", lots - 1)))
    squares = end(mate_d, squares)

    inverse = lax.rsqrt(squares * (1.0 / (columns_each * dp)) + EPSILON)
    for j in range(dp):
        columns = slice(j * columns_each, (j + 1) * columns_each)
        out_ref[:, columns] = (proj[:, columns] * inverse * og_ref[:, columns]).astype(BF16)

    for copy in sent:
        copy.wait_send()
    for name in ("x", "y"):
        w_share_sent(name)
    for step in range(sp - 1):
        for way in (0, 1):
            @pl.when(kv_sends(way, step))
            def _(way=way, step=step):
                for kind in (0, 1):
                    for side in range(HALVES):
                        kv_copy(way, step, kind, side).wait_send()


def per_device_fused(sp, dp, queries, keys, values, query_gain, key_gain, out_weight, out_gain):
    tokens = queries.shape[1]
    depth, columns = out_weight.shape
    hidden = queries.shape[2]
    kv_width = keys.shape[2]
    seq_len = tokens * sp
    hbm_spec = pl.BlockSpec(memory_space=pltpu.HBM)
    vmem_spec = pl.BlockSpec(memory_space=pltpu.VMEM)
    result = pl.pallas_call(
        functools.partial(kernel, sp, dp),
        out_shape=pltpu.VMEM((tokens, columns * dp), BF16),
        in_specs=[hbm_spec] * 3 + [vmem_spec] * 2 + [hbm_spec, vmem_spec, hbm_spec],
        out_specs=vmem_spec,
        scratch_shapes=[
            pltpu.VMEM((tokens, hidden), BF16),
            pltpu.VMEM((seq_len, kv_width), BF16),
            pltpu.VMEM((seq_len, kv_width), BF16),
            pltpu.VMEM((2, seq_len, 2 * HEAD), F32),
            pltpu.VMEM((dp, depth, columns), BF16),
            pltpu.VMEM((4, 16, BLOCK), F32),
            pltpu.VMEM((BLOCK, BLOCK), BF16),
            pltpu.VMEM((BLOCK, BLOCK), BF16),
            pltpu.VMEM((KVH, kv_width // HALVES, GROUP * tokens), BF16),
            pltpu.VMEM((kv_width, seq_len), BF16),
            pltpu.VMEM((sp - 1, KVH, tokens, GROUP * tokens), F32),
            pltpu.VMEM((sp - 1, KVH, 1, GROUP * tokens), F32),
            pltpu.VMEM((sp - 1, KVH, 1, GROUP * tokens), F32),
            pltpu.VMEM((KVH, seq_len, GROUP * tokens), BF16),
            pltpu.VMEM((tokens, hidden), BF16),
            pltpu.VMEM((tokens, columns * dp), F32),
            pltpu.SemaphoreType.DMA((5,)),
            pltpu.SemaphoreType.DMA((2, sp - 1, HALVES, 2)),
            pltpu.SemaphoreType.DMA((2, sp - 1, HALVES, 2)),
            pltpu.SemaphoreType.DMA((PIECES,)),
            pltpu.SemaphoreType.DMA((PIECES,)),
        ],
        compiler_params=pltpu.CompilerParams(
            collective_id=0, has_side_effects=True, vmem_limit_bytes=66000000
        ),
    )(
        queries[0], keys[0], values[0], query_gain[None], key_gain[None],
        out_weight, out_gain[None], jnp.asarray(position_tables(seq_len)),
    )
    return result[None]


def solution(mesh):
    sp, dp = mesh.shape["sp"], mesh.shape["dp"]
    if dp == 8 and sp >= 2 and sp % 2 == 0 and sp <= 4:
        body = functools.partial(per_device_fused, sp, dp)
    else:
        body = per_device_general
    return jax.shard_map(
        body,
        mesh=mesh,
        in_specs=(
            P("dp", "sp", None),
            P("dp", "sp", None),
            P("dp", "sp", None),
            P(),
            P(),
            P(None, "dp"),
            P(),
        ),
        out_specs=P("dp", "sp", None),
        check_vma=False,
    )
```

```python
import functools

import jax
import jax.numpy as jnp
import numpy as np
from jax import lax
from jax.experimental import pallas as pl
from jax.experimental.pallas import tpu as pltpu
from jax.sharding import PartitionSpec as P

QH = 16
KVH = 4
HEAD = 64
GRID_W = 64
GROUP = QH // KVH
HALVES = 2
BLOCK = GROUP * HEAD
WIDTH = 128

TO_END = 128
TO_INNER = 160
CHUNKS = (256, 128, 128)
LATE = 128
PIECES = 8 * len(CHUNKS) + 17


EPSILON = 1e-06
ROTARY_BASE = 10000.0

F32 = jnp.float32
BF16 = jnp.bfloat16


def rotate(vectors, positions, width):
    half_width = width // 2
    frequency = ROTARY_BASE ** (-jnp.arange(0, width, 2, dtype=jnp.float32) / width)
    angles = positions.astype(jnp.float32)[:, None] * frequency[None, :]
    cosines = jnp.cos(angles)[:, None, :]
    sine_table = jnp.sin(angles)[:, None, :]
    first_half = vectors[..., :half_width]
    second_half = vectors[..., half_width:]
    return jnp.concatenate(
        [
            first_half * cosines - second_half * sine_table,
            second_half * cosines + first_half * sine_table,
        ],
        axis=-1,
    )


def prepare(vectors, gain_vector, grid_row, grid_col):
    vectors = vectors.astype(jnp.float32)
    vectors = (
        vectors
        * lax.rsqrt(jnp.mean(vectors * vectors, axis=-1, keepdims=True) + EPSILON)
        * gain_vector
    )
    half_width = HEAD // 2
    turned = jnp.concatenate(
        [
            rotate(vectors[..., :half_width], grid_row, half_width),
            rotate(vectors[..., half_width:], grid_col, half_width),
        ],
        axis=-1,
    )
    return turned.astype(jnp.bfloat16)


def softmax_rows(scores):
    row_max = jnp.max(scores, axis=-1, keepdims=True)
    exponent = jnp.exp(scores - row_max)
    return exponent / jnp.sum(exponent, axis=-1, keepdims=True)


def per_device_general(queries, keys, values, query_gain, key_gain, out_weight, out_gain):
    sp_count = lax.axis_size("sp")
    tokens_here = queries.shape[1]
    seq_len = tokens_here * sp_count
    score_scale = HEAD ** (-0.5)
    offset = lax.axis_index("sp") * tokens_here
    positions = offset + jnp.arange(tokens_here, dtype=jnp.int32)
    grid_row = positions // GRID_W
    grid_col = positions % GRID_W
    query_rot = prepare(queries[0].reshape(tokens_here, QH, HEAD), query_gain, grid_row, grid_col)
    key_rot = prepare(keys[0].reshape(tokens_here, KVH, HEAD), key_gain, grid_row, grid_col)
    value_heads = values[0].reshape(tokens_here, KVH, HEAD)
    kv_pairs = jnp.concatenate([key_rot, value_heads], axis=2)
    all_pairs = lax.all_gather(
        kv_pairs.reshape(tokens_here, KVH * 2 * HEAD), "sp", axis=0, tiled=True
    )
    all_pairs = all_pairs.reshape(seq_len, KVH, 2, HEAD)
    key_all = all_pairs[:, :, 0].transpose(1, 0, 2)
    value_all = all_pairs[:, :, 1].transpose(1, 0, 2)
    query_groups = query_rot.reshape(tokens_here, KVH, QH // KVH, HEAD).transpose(1, 0, 2, 3)

    def attend_group(operands):
        query_group, key_head, value_head = operands
        scores = (
            jnp.einsum("qgd,kd->gqk", query_group, key_head, preferred_element_type=jnp.float32)
            * score_scale
        )
        attn_weights = softmax_rows(scores).astype(jnp.bfloat16)
        return jnp.einsum(
            "gqk,kd->qgd", attn_weights, value_head, preferred_element_type=jnp.float32
        ).astype(jnp.bfloat16)

    results = lax.map(attend_group, (query_groups, key_all, value_all))
    attended = results.transpose(1, 0, 2, 3).reshape(tokens_here, QH * HEAD)
    projected = jnp.dot(
        attended,
        lax.all_gather(out_weight, "dp", axis=1, tiled=True),
        preferred_element_type=jnp.float32,
    )
    normed = (
        projected
        * lax.rsqrt(jnp.mean(projected * projected, axis=-1, keepdims=True) + EPSILON)
        * out_gain
    )
    return normed.astype(jnp.bfloat16)[None]


def position_tables(seq_len):
    width = HEAD // 2
    frequency = np.float32(ROTARY_BASE) ** (
        -np.arange(0, width, 2, dtype=np.float32) / np.float32(width)
    )
    position = np.arange(seq_len)
    parts = []
    for coordinate in (position // GRID_W, position % GRID_W):
        angles = coordinate.astype(np.float32)[:, None] * frequency[None, :]
        parts += [angles, angles]
    angles = np.concatenate(parts * 2, axis=1).astype(np.float64)
    return np.stack([np.cos(angles), np.sin(angles)]).astype(np.float32)


def dot(a, b):
    return jnp.dot(a, b, preferred_element_type=F32)


def cross(a, b):
    return lax.dot_general(a, b, (((1,), (1,)), ((), ())), preferred_element_type=F32)


def kernel(
    sp, dp,
    q_ref, k_ref, v_ref, qg_hbm, kg_hbm, w_ref, og_hbm, table_ref,
    out_ref,
    q_raw, k_all, v_all, tables, w_all, gains,
    swap_mat, ones_mat, q_t, v_turned, v_last, partial,
    expo, peak, total, mixed, att, proj,
    qg_ref, kg_ref, og_ref, local_sem, kv_send, kv_recv, w_send, w_recv,
):
    tokens = q_raw.shape[0]
    depth = w_ref.shape[0]
    half = depth // 2
    me = lax.axis_index("sp")
    here = lax.axis_index("dp")
    mate = here + 1 - 2 * (here % 2)
    flip_x = 2 - 4 * ((here // 2) % 2)
    flip_y = 4 - 8 * ((here // 4) % 2)
    dev_x = here + flip_x
    dev_y = here + flip_y
    dev_d = here + flip_x + flip_y

    barrier = pltpu.get_barrier_semaphore()
    has_left = me > 0
    has_right = me < sp - 1

    for other in (mate, dev_x, dev_y):
        pl.semaphore_signal(barrier, inc=1, device_id={"dp": other})

    @pl.when(has_left)
    def _():
        pl.semaphore_signal(barrier, inc=1, device_id={"sp": me - 1})

    @pl.when(has_right)
    def _():
        pl.semaphore_signal(barrier, inc=1, device_id={"sp": me + 1})

    locals_ = [
        pltpu.make_async_copy(k_ref, k_all.at[pl.ds(me * tokens, tokens)], local_sem.at[0]),
        pltpu.make_async_copy(v_ref, v_all.at[pl.ds(me * tokens, tokens)], local_sem.at[1]),
        pltpu.make_async_copy(w_ref, w_all.at[here], local_sem.at[2]),
        pltpu.make_async_copy(q_ref, q_raw, local_sem.at[3]),
        pltpu.make_async_copy(table_ref, tables, local_sem.at[4]),
        pltpu.make_async_copy(qg_hbm, qg_ref, local_sem.at[5]),
        pltpu.make_async_copy(kg_hbm, kg_ref, local_sem.at[6]),
        pltpu.make_async_copy(og_hbm, og_ref, local_sem.at[7]),
    ]
    for copy in locals_:
        copy.start()

    row_id = lax.broadcasted_iota(jnp.int32, (BLOCK, BLOCK), 0)
    col_id = lax.broadcasted_iota(jnp.int32, (BLOCK, BLOCK), 1)
    quarter = HEAD // 4
    second = (col_id & (HEAD // 2 - 1)) >= quarter
    partner_col = jnp.where(second, col_id - quarter, col_id + quarter)
    hit = row_id == partner_col
    swap_mat[...] = jnp.where(hit, jnp.where(second, 1.0, -1.0), 0.0).astype(BF16)
    ones_mat[...] = jnp.where((row_id // HEAD) == (col_id // HEAD), 1.0, 0.0).astype(BF16)
    spread = jnp.where(
        row_id[:HEAD] == (col_id[:HEAD] & (HEAD - 1)), 1.0, 0.0
    ).astype(BF16)
    spread_swapped = jnp.where(
        row_id[:HEAD] == (partner_col[:HEAD] & (HEAD - 1)), 1.0, 0.0
    ).astype(BF16)
    lane_head = lax.broadcasted_iota(jnp.int32, (1, BLOCK), 1) // HEAD
    masks = [jnp.where(lane_head == p, 1.0, 0.0).astype(BF16) for p in range(GROUP)]

    pl.semaphore_wait(barrier, 3 + jnp.minimum(me, 1) + jnp.minimum(sp - 1 - me, 1))

    part = k_ref.shape[1] // HALVES

    stores = (k_all, v_all)
    owns = (k_ref, v_ref)

    def kv_copy(way, step, kind, side):
        block = me - step if way == 0 else me + step
        target = me + 1 if way == 0 else me - 1
        columns = pl.ds(side * part, part)
        window = stores[kind].at[pl.ds(block * tokens, tokens), columns]
        return pltpu.make_async_remote_copy(
            src_ref=owns[kind].at[:, columns] if step == 0 else window,
            dst_ref=window,
            send_sem=kv_send.at[way, step, side, kind],
            recv_sem=kv_recv.at[way, step, side, kind],
            device_id={"sp": target},
        )

    def kv_sends(way, step):
        if way == 0:
            return jnp.logical_and(has_right, me - step >= 0)
        return jnp.logical_and(has_left, me + step < sp)

    def kv_start(way, step, kind, side):
        @pl.when(kv_sends(way, step))
        def _():
            kv_copy(way, step, kind, side).start()

    def kv_arrive(step, kind, side):
        for way in (0, 1):
            source = me - 1 - step if way == 0 else me + 1 + step
            arrives = source >= 0 if way == 0 else source < sp

            @pl.when(arrives)
            def _(way=way, source=source):
                window = stores[kind].at[
                    pl.ds(source * tokens, tokens), pl.ds(side * part, part)
                ]
                pltpu.make_async_remote_copy(
                    src_ref=window,
                    dst_ref=window,
                    send_sem=kv_send.at[way, step, side, kind],
                    recv_sem=kv_recv.at[way, step, side, kind],
                    device_id={"sp": me},
                ).wait_recv()

            if step + 1 < sp - 1:
                kv_start(way, step + 1, kind, side)

    for kind in (0, 1):
        for side in range(HALVES):
            for way in (1, 0):
                kv_start(way, 0, kind, side)

    odd = me % 2
    zmate = me + 1 - 2 * odd
    inner = (me + 1) // 2 % 2 == 1
    outer = jnp.logical_not(inner)
    shares = ((inner, 0, TO_END), (outer, half - TO_INNER, TO_INNER))
    mate_x, mate_y, mate_d = mate + flip_x, mate + flip_y, mate + flip_x + flip_y

    starts = [sum(CHUNKS[:j]) for j in range(len(CHUNKS))]
    pieces = {"own": (mate, 0, depth)}
    for j, (start, size) in enumerate(zip(starts, CHUNKS)):
        pieces["x", j] = (dev_x, half + start, size)
        pieces["y", j] = (dev_y, start, size)
        pieces["dx", j] = (dev_d, start, size)
        pieces["dy", j] = (dev_d, half + start, size)
    for name, shard, base in (("x", dev_x, 0), ("y", dev_y, half)):
        pieces[name, "middle"] = (shard, base + TO_END, half - TO_END - TO_INNER)
        for role, (_, start, size) in enumerate(shares):
            pieces[name, "share", role] = (shard, base + start, size)
    across = {"x": mate_x, "y": mate_y, "dx": mate_d, "dy": mate_d}
    for name in [name for name in pieces if name != "own"]:
        start, size = pieces[name][1:]
        pieces["mate", name] = (across[name[0]], start, size)
        if name[1] == "share":
            pieces["zed", name] = pieces[name]
    order = {name: i for i, name in enumerate(pieces)}
    sent = []

    def w_copy(name, shard, start, size, target, own=False):
        window = w_all.at[shard, pl.ds(start, size)]
        return pltpu.make_async_remote_copy(
            src_ref=w_ref.at[pl.ds(start, size)] if own else window,
            dst_ref=window,
            send_sem=w_send.at[order[name]],
            recv_sem=w_recv.at[order[name]],
            device_id=target,
        )

    def w_give(name, shard, start, size, target, own=False):
        copy = w_copy(name, shard, start, size, target, own)
        copy.start()
        sent.append(copy)

    def w_own(name, target):
        w_give(name, here, *pieces[name][1:], {"dp": target}, own=True)

    def w_wait(name):
        w_copy(name, *pieces[name], {"dp": mate}).wait_recv()

    def w_take(name):
        w_wait(name)
        piece = pieces[name]
        if name[1] in range(len(CHUNKS)):
            if name[0] == "x":
                w_give(("dy", name[1]), *piece, {"dp": dev_y})
            if name[0] == "y":
                w_give(("dx", name[1]), *piece, {"dp": dev_x})
        w_give(("mate", name), *piece, {"dp": mate})

    def w_share_own(name):
        for role, (chosen, _, _) in enumerate(shares):
            @pl.when(chosen)
            def _(key=(name, "share", role)):
                target = dev_x if name == "x" else dev_y
                w_copy(key, here, *pieces[key][1:], {"dp": target}, own=True).start()

    def w_share_near(role):
        @pl.when(shares[role][0])
        def _():
            for name in ("x", "y"):
                key = (name, "share", role)
                w_wait(key)
                w_copy(("zed", key), *pieces[key], {"sp": zmate}).start()
                w_copy(("mate", key), *pieces[key], {"dp": mate}).start()

    def w_share_far(role):
        @pl.when(shares[1 - role][0])
        def _():
            for name in ("x", "y"):
                key = (name, "share", role)
                w_wait(("zed", key))
                w_copy(("mate", key), *pieces[key], {"dp": mate}).start()

    def w_share_sent(name):
        for role, (chosen, _, _) in enumerate(shares):
            key = (name, "share", role)
            w_copy(("mate", key), *pieces[key], {"dp": mate}).wait_send()

            @pl.when(chosen)
            def _(key=key):
                for form in (key, ("zed", key)):
                    w_copy(form, *pieces[key], {"dp": mate}).wait_send()

    for j in range(len(CHUNKS)):
        w_own(("x", j), dev_x)
        w_own(("y", j), dev_y)
    w_share_own("x")
    w_share_own("y")
    w_own(("x", "middle"), dev_x)
    w_own(("y", "middle"), dev_y)
    w_own("own", mate)

    def turned(x, rows, which, scale):
        xf = x.astype(F32)
        square = xf * xf
        high = square.astype(BF16)
        low = (square - high.astype(F32)).astype(BF16)
        size = x.shape[1]
        ones = ones_mat[:size, :size]
        mean = (dot(high, ones) + dot(low, ones)) * (1.0 / HEAD)
        inverse = lax.rsqrt(mean + EPSILON) * scale
        swapped = dot(x, swap_mat[:size, :size])
        cosines = tables[0, rows, :]
        sines = tables[1, rows, :]
        if size > 2 * HEAD:
            cosines = jnp.concatenate([cosines, cosines], axis=1)
            sines = jnp.concatenate([sines, sines], axis=1)
        cosines = cosines * gains[2 * which, 0:1, :size]
        sines = sines * gains[2 * which + 1, 0:1, :size]
        return ((xf * cosines + swapped * sines) * inverse).astype(BF16)

    locals_[5].wait()
    locals_[6].wait()
    for i, gain_ref in enumerate((qg_ref, kg_ref)):
        gain = jnp.broadcast_to(gain_ref[...], (16, HEAD))
        first = gain.astype(BF16)
        rest = gain - first.astype(F32)
        mid = rest.astype(BF16)
        low = (rest - mid.astype(F32)).astype(BF16)
        for j, matrix in enumerate((spread, spread_swapped)):
            gains[2 * i + j] = (dot(first, matrix) + dot(mid, matrix)) + dot(low, matrix)

    locals_[3].wait()
    locals_[4].wait()
    locals_[7].wait()
    own_rows = pl.ds(pl.multiple_of(me * tokens, 64), tokens)
    for b in range(KVH):
        columns = slice(b * BLOCK, (b + 1) * BLOCK)
        query = turned(q_raw[:, columns], own_rows, 0, HEAD ** (-0.5))
        parts = [query[:WIDTH] * mask for mask in masks] + [query[WIDTH:] * mask for mask in masks]
        held = b % 2 * HEAD
        fold = jnp.where(row_id[:part] - held == (col_id[:part] & (HEAD - 1)), 1.0, 0.0)
        q_t[b] = cross(fold.astype(BF16), jnp.concatenate(parts, axis=0)).astype(BF16)

    eye = jnp.where(row_id == col_id, 1.0, 0.0).astype(BF16)
    far = 1 - me // 2
    blocks = [me, zmate, far + 1, 3 * far][:sp]
    spans = [pl.ds(pl.multiple_of(block * tokens, 64), tokens) for block in blocks]
    heads = KVH // HALVES
    rest = tokens - WIDTH
    final = sp - 1

    def score(turn, side):
        lanes = slice(side * part, (side + 1) * part)
        rows = spans[turn]
        key_side = turned(k_all[rows, lanes], rows, 1, 1.0)
        for b in range(side * heads, (side + 1) * heads):
            scores = dot(key_side, q_t[b])
            high = jnp.max(scores, axis=0, keepdims=True)
            if turn < final:
                weights = jnp.exp(scores - high)
                expo[turn, b] = weights
                peak[turn, b] = high
                total[turn, b] = jnp.sum(weights, axis=0, keepdims=True)
                continue
            for t in range(turn):
                high = jnp.maximum(high, peak[t, b])
            weights = jnp.exp(scores - high)
            norm = jnp.sum(weights, axis=0, keepdims=True)
            keeps = [jnp.exp(peak[t, b] - high) for t in range(turn)]
            for t in range(turn):
                norm = norm + total[t, b] * keeps[t]
            inverse = 1.0 / norm
            for t in range(turn):
                mixed[b, t * tokens : (t + 1) * tokens, :] = (
                    expo[t, b] * (keeps[t] * inverse)
                ).astype(BF16)
            mixed[b, turn * tokens :, :] = (weights * inverse).astype(BF16)

    def values(blocks, side):
        lanes = slice(side * part, (side + 1) * part)
        stack = jnp.concatenate([v_all[spans[t], lanes] for t in blocks], axis=0)
        result = cross(eye[:part, :part], stack).astype(BF16)
        if blocks[0] == final:
            v_last[lanes, :] = result
        else:
            v_turned[lanes, blocks[0] * tokens : (blocks[-1] + 1) * tokens] = result

    def each_head(side):
        for b in range(side * heads, (side + 1) * heads):
            yield b, slice(b * HEAD, (b + 1) * HEAD)

    def early(side):
        for b, value_rows in each_head(side):
            partial[b] = dot(v_turned[value_rows, :], mixed[b, : final * tokens, :])

    def gather(side):
        for b, value_rows in each_head(side):
            product = partial[b] + dot(v_last[value_rows, :], mixed[b, final * tokens :, :])
            for p in range(0, GROUP, 2):
                lanes = slice(b * BLOCK + p * HEAD, b * BLOCK + (p + 2) * HEAD)
                two = [product[:, i * WIDTH : (i + 1) * WIDTH] for i in (p, p + 1)]
                att[:WIDTH, lanes] = jnp.concatenate(two, axis=0).T.astype(BF16)
                start = GROUP * WIDTH + p * rest
                two = product[:, start : start + 2 * rest].T
                two = jnp.concatenate([two[:rest], two[rest:]], axis=1)
                att[WIDTH:, lanes] = two.astype(BF16)

    lots = len(CHUNKS)
    columns_each = w_ref.shape[1]
    late = LATE
    tails = {2: [0], 3: [half], 4: [0], 5: [half]}
    tails[6] = tails[7] = [half - late, depth - late]

    def columns_of(shard):
        return pl.ds(pl.multiple_of(shard * columns_each, columns_each), columns_each)

    def product(shard, start, size):
        rows = pl.ds(start, size)
        return dot(att[:, rows], w_all[shard, rows, :])

    def squares_of(result):
        square = result * result
        return sum(square[:, i : i + 128] for i in range(0, columns_each, 128))

    slots = [here, mate, dev_x, dev_y, mate_x, mate_y, dev_d, mate_d]

    def project(slot, squares):
        shard = slots[slot]
        result = dot(att[...], w_all[shard])
        proj[slot] = result * og_ref[:, columns_of(shard)]
        return squares + squares_of(result)

    def begin(slot):
        done, result = 0, 0.0
        for start in [*tails[slot], depth]:
            if start > done:
                result = result + product(slots[slot], done, start - done)
            done = start + late
        proj[slot] = result

    def end(slot):
        result = proj[slot]
        for start in tails[slot]:
            result = result + product(slots[slot], start, late)
        return result

    def end_early(slot, squares):
        result = end(slot)
        proj[slot] = result * og_ref[:, columns_of(slots[slot])]
        return squares + squares_of(result)

    def take(*names):
        for name in names:
            w_take(("x", name))
            w_take(("y", name))

    def take_far(j):
        w_take(("dx", j))
        w_take(("dy", j))

    locals_[0].wait()
    for side in range(HALVES):
        score(0, side)
    locals_[1].wait()

    jobs = {
        (0, 1, 0): lambda: take(0),
        (0, 1, 1): lambda: take(1),
        (1, 0, 0): lambda: take(*range(2, lots)),
        (1, 1, 0): lambda: w_share_near(1),
        (1, 1, 1): lambda: w_share_near(0),
        (2, 0, 0): lambda: take("middle"),
    }
    for step in range(sp - 1):
        turn = step + 1
        for kind in (0, 1):
            for side in range(HALVES):
                kv_arrive(step, kind, side)
                if kind == 0:
                    score(turn, side)
                    if turn == final:
                        if turn == 1:
                            values([0], side)
                        early(side)
                elif turn == final:
                    values([final], side)
                    gather(side)
                    if side == 0:
                        take_far(0)
                elif turn == 1:
                    values([0, 1], side)
                else:
                    values([turn], side)
                if (step, kind, side) in jobs:
                    jobs.pop((step, kind, side))()
    for job in jobs.values():
        job()

    w_share_far(1)
    locals_[2].wait()
    squares = project(0, jnp.zeros((tokens, 128), F32))
    w_wait("own")
    squares = project(1, squares)
    begin(2)
    begin(3)
    for j in range(1, lots - 1):
        take_far(j)
    for slot, name in ((4, "x"), (5, "y")):
        for piece in (*range(lots), "middle"):
            w_wait(("mate", (name, piece)))
        w_wait(("mate", (name, "share", 1)))
        begin(slot)
    begin(6)
    w_share_far(0)
    take_far(lots - 1)
    for slot in (2, 3):
        squares = end_early(slot, squares)
    for j in range(lots - 1):
        w_wait(("mate", ("dx", j)))
        w_wait(("mate", ("dy", j)))
    begin(7)
    for slot, name in ((4, "x"), (5, "y")):
        w_wait(("mate", (name, "share", 0)))
        squares = end_early(slot, squares)
    for axis in ("dx", "dy"):
        w_wait(("mate", (axis, lots - 1)))
    ends = [end(6), end(7)]
    for result in ends:
        squares = squares + squares_of(result)
    squares = jnp.sum(squares, axis=1, keepdims=True)
    inverse = lax.rsqrt(squares * (1.0 / (columns_each * dp)) + EPSILON)
    for slot, shard in enumerate(slots):
        columns = columns_of(shard)
        if slot < 6:
            result = proj[slot]
        else:
            result = ends[slot - 6] * og_ref[:, columns]
        out_ref[:, columns] = (result * inverse).astype(BF16)

    for copy in sent:
        copy.wait_send()
    for name in ("x", "y"):
        w_share_sent(name)
    for step in range(sp - 1):
        for way in (0, 1):
            @pl.when(kv_sends(way, step))
            def _(way=way, step=step):
                for kind in (0, 1):
                    for side in range(HALVES):
                        kv_copy(way, step, kind, side).wait_send()


def per_device_fused(sp, dp, queries, keys, values, query_gain, key_gain, out_weight, out_gain):
    tokens = queries.shape[1]
    depth, columns = out_weight.shape
    hidden = queries.shape[2]
    kv_width = keys.shape[2]
    seq_len = tokens * sp
    hbm_spec = pl.BlockSpec(memory_space=pltpu.HBM)
    vmem_spec = pl.BlockSpec(memory_space=pltpu.VMEM)
    result = pl.pallas_call(
        functools.partial(kernel, sp, dp),
        out_shape=pltpu.VMEM((tokens, columns * dp), BF16),
        in_specs=[hbm_spec] * 8,
        out_specs=vmem_spec,
        scratch_shapes=[
            pltpu.VMEM((tokens, hidden), BF16),
            pltpu.VMEM((seq_len, kv_width), BF16),
            pltpu.VMEM((seq_len, kv_width), BF16),
            pltpu.VMEM((2, seq_len, 2 * HEAD), F32),
            pltpu.VMEM((dp, depth, columns), BF16),
            pltpu.VMEM((4, 16, BLOCK), F32),
            pltpu.VMEM((BLOCK, BLOCK), BF16),
            pltpu.VMEM((BLOCK, BLOCK), BF16),
            pltpu.VMEM((KVH, kv_width // HALVES, GROUP * tokens), BF16),
            pltpu.VMEM((kv_width, seq_len - tokens), BF16),
            pltpu.VMEM((kv_width, tokens), BF16),
            pltpu.VMEM((KVH, HEAD, GROUP * tokens), F32),
            pltpu.VMEM((sp - 1, KVH, tokens, GROUP * tokens), F32),
            pltpu.VMEM((sp - 1, KVH, 1, GROUP * tokens), F32),
            pltpu.VMEM((sp - 1, KVH, 1, GROUP * tokens), F32),
            pltpu.VMEM((KVH, seq_len, GROUP * tokens), BF16),
            pltpu.VMEM((tokens, hidden), BF16),
            pltpu.VMEM((dp, tokens, columns), F32),
            pltpu.VMEM((1, HEAD), F32),
            pltpu.VMEM((1, HEAD), F32),
            pltpu.VMEM((1, columns * dp), F32),
            pltpu.SemaphoreType.DMA((8,)),
            pltpu.SemaphoreType.DMA((2, sp - 1, HALVES, 2)),
            pltpu.SemaphoreType.DMA((2, sp - 1, HALVES, 2)),
            pltpu.SemaphoreType.DMA((PIECES,)),
            pltpu.SemaphoreType.DMA((PIECES,)),
        ],
        compiler_params=pltpu.CompilerParams(
            collective_id=0, has_side_effects=True, vmem_limit_bytes=66000000
        ),
    )(
        queries[0], keys[0], values[0], query_gain[None], key_gain[None],
        out_weight, out_gain[None], jnp.asarray(position_tables(seq_len)),
    )
    return result[None]


def solution(mesh):
    sp, dp = mesh.shape["sp"], mesh.shape["dp"]
    if dp == 8 and sp >= 2 and sp % 2 == 0 and sp <= 4:
        body = functools.partial(per_device_fused, sp, dp)
    else:
        body = per_device_general
    return jax.shard_map(
        body,
        mesh=mesh,
        in_specs=(
            P("dp", "sp", None),
            P("dp", "sp", None),
            P("dp", "sp", None),
            P(),
            P(),
            P(None, "dp"),
            P(),
        ),
        out_specs=P("dp", "sp", None),
        check_vma=False,
    )
```

```python
import functools

import jax
import jax.numpy as jnp
import numpy as np
from jax import lax
from jax.experimental import pallas as pl
from jax.experimental.pallas import tpu as pltpu
from jax.sharding import PartitionSpec as P

QH = 16
KVH = 4
HEAD = 64
GRID_W = 64
GROUP = QH // KVH
HALVES = 2
BLOCK = GROUP * HEAD
WIDTH = 128

TO_END = 128
TO_INNER = 192
CHUNKS = (256, 128, 128)
LATE = 128
PIECES = 8 * len(CHUNKS) + 17


EPSILON = 1e-06
ROTARY_BASE = 10000.0

F32 = jnp.float32
BF16 = jnp.bfloat16


def rotate(vectors, positions, width):
    half_width = width // 2
    frequency = ROTARY_BASE ** (-jnp.arange(0, width, 2, dtype=jnp.float32) / width)
    angles = positions.astype(jnp.float32)[:, None] * frequency[None, :]
    cosines = jnp.cos(angles)[:, None, :]
    sine_table = jnp.sin(angles)[:, None, :]
    first_half = vectors[..., :half_width]
    second_half = vectors[..., half_width:]
    return jnp.concatenate(
        [
            first_half * cosines - second_half * sine_table,
            second_half * cosines + first_half * sine_table,
        ],
        axis=-1,
    )


def prepare(vectors, gain_vector, grid_row, grid_col):
    vectors = vectors.astype(jnp.float32)
    vectors = (
        vectors
        * lax.rsqrt(jnp.mean(vectors * vectors, axis=-1, keepdims=True) + EPSILON)
        * gain_vector
    )
    half_width = HEAD // 2
    turned = jnp.concatenate(
        [
            rotate(vectors[..., :half_width], grid_row, half_width),
            rotate(vectors[..., half_width:], grid_col, half_width),
        ],
        axis=-1,
    )
    return turned.astype(jnp.bfloat16)


def softmax_rows(scores):
    row_max = jnp.max(scores, axis=-1, keepdims=True)
    exponent = jnp.exp(scores - row_max)
    return exponent / jnp.sum(exponent, axis=-1, keepdims=True)


def per_device_general(queries, keys, values, query_gain, key_gain, out_weight, out_gain):
    sp_count = lax.axis_size("sp")
    tokens_here = queries.shape[1]
    seq_len = tokens_here * sp_count
    score_scale = HEAD ** (-0.5)
    offset = lax.axis_index("sp") * tokens_here
    positions = offset + jnp.arange(tokens_here, dtype=jnp.int32)
    grid_row = positions // GRID_W
    grid_col = positions % GRID_W
    query_rot = prepare(queries[0].reshape(tokens_here, QH, HEAD), query_gain, grid_row, grid_col)
    key_rot = prepare(keys[0].reshape(tokens_here, KVH, HEAD), key_gain, grid_row, grid_col)
    value_heads = values[0].reshape(tokens_here, KVH, HEAD)
    kv_pairs = jnp.concatenate([key_rot, value_heads], axis=2)
    all_pairs = lax.all_gather(
        kv_pairs.reshape(tokens_here, KVH * 2 * HEAD), "sp", axis=0, tiled=True
    )
    all_pairs = all_pairs.reshape(seq_len, KVH, 2, HEAD)
    key_all = all_pairs[:, :, 0].transpose(1, 0, 2)
    value_all = all_pairs[:, :, 1].transpose(1, 0, 2)
    query_groups = query_rot.reshape(tokens_here, KVH, QH // KVH, HEAD).transpose(1, 0, 2, 3)

    def attend_group(operands):
        query_group, key_head, value_head = operands
        scores = (
            jnp.einsum("qgd,kd->gqk", query_group, key_head, preferred_element_type=jnp.float32)
            * score_scale
        )
        attn_weights = softmax_rows(scores).astype(jnp.bfloat16)
        return jnp.einsum(
            "gqk,kd->qgd", attn_weights, value_head, preferred_element_type=jnp.float32
        ).astype(jnp.bfloat16)

    results = lax.map(attend_group, (query_groups, key_all, value_all))
    attended = results.transpose(1, 0, 2, 3).reshape(tokens_here, QH * HEAD)
    projected = jnp.dot(
        attended,
        lax.all_gather(out_weight, "dp", axis=1, tiled=True),
        preferred_element_type=jnp.float32,
    )
    normed = (
        projected
        * lax.rsqrt(jnp.mean(projected * projected, axis=-1, keepdims=True) + EPSILON)
        * out_gain
    )
    return normed.astype(jnp.bfloat16)[None]


def position_tables(seq_len):
    width = HEAD // 2
    frequency = np.float32(ROTARY_BASE) ** (
        -np.arange(0, width, 2, dtype=np.float32) / np.float32(width)
    )
    position = np.arange(seq_len)
    parts = []
    for coordinate in (position // GRID_W, position % GRID_W):
        angles = coordinate.astype(np.float32)[:, None] * frequency[None, :]
        parts += [angles, angles]
    angles = np.concatenate(parts * 2, axis=1).astype(np.float64)
    return np.stack([np.cos(angles), np.sin(angles)]).astype(np.float32)


def dot(a, b):
    return jnp.dot(a, b, preferred_element_type=F32)


def cross(a, b):
    return lax.dot_general(a, b, (((1,), (1,)), ((), ())), preferred_element_type=F32)


def kernel(
    sp, dp,
    q_ref, k_ref, v_ref, qg_hbm, kg_hbm, w_ref, og_hbm, table_ref,
    out_ref,
    q_raw, k_all, v_all, tables, w_all, gains,
    swap_mat, ones_mat, q_t, v_turned, v_last, partial,
    expo, peak, total, mixed, att, proj,
    qg_ref, kg_ref, og_ref, above, local_sem, kv_send, kv_recv, w_send, w_recv,
):
    tokens = q_raw.shape[0]
    depth = w_ref.shape[0]
    half = depth // 2
    me = lax.axis_index("sp")
    here = lax.axis_index("dp")
    mate = here + 1 - 2 * (here % 2)
    flip_x = 2 - 4 * ((here // 2) % 2)
    flip_y = 4 - 8 * ((here // 4) % 2)
    dev_x = here + flip_x
    dev_y = here + flip_y
    dev_d = here + flip_x + flip_y

    barrier = pltpu.get_barrier_semaphore()
    has_left = me > 0
    has_right = me < sp - 1

    low_x, low_y = (here // 2) % 2 == 0, (here // 4) % 2 == 0
    high_x, high_y = jnp.logical_not(low_x), jnp.logical_not(low_y)
    ways = (
        (low_x, high_x, {"dp": dev_x}, {"dp": dev_x}),
        (low_y, high_y, {"dp": dev_y}, {"dp": dev_y}),
        (has_right, has_left, {"sp": me + 1}, {"sp": me - 1}),
    )

    pl.semaphore_signal(barrier, inc=1, device_id={"dp": mate})
    for up, _, target, _ in ways:
        @pl.when(up)
        def _(target=target):
            pl.semaphore_signal(barrier, inc=1, device_id=target)

    locals_ = [
        pltpu.make_async_copy(k_ref, k_all.at[pl.ds(me * tokens, tokens)], local_sem.at[0]),
        pltpu.make_async_copy(v_ref, v_all.at[pl.ds(me * tokens, tokens)], local_sem.at[1]),
        pltpu.make_async_copy(w_ref, w_all.at[here], local_sem.at[2]),
        pltpu.make_async_copy(q_ref, q_raw, local_sem.at[3]),
        pltpu.make_async_copy(table_ref, tables, local_sem.at[4]),
        pltpu.make_async_copy(qg_hbm, qg_ref, local_sem.at[5]),
        pltpu.make_async_copy(kg_hbm, kg_ref, local_sem.at[6]),
        pltpu.make_async_copy(og_hbm, og_ref, local_sem.at[7]),
    ]
    for copy in locals_:
        copy.start()

    row_id = lax.broadcasted_iota(jnp.int32, (BLOCK, BLOCK), 0)
    col_id = lax.broadcasted_iota(jnp.int32, (BLOCK, BLOCK), 1)
    quarter = HEAD // 4
    second = (col_id & (HEAD // 2 - 1)) >= quarter
    partner_col = jnp.where(second, col_id - quarter, col_id + quarter)
    hit = row_id == partner_col
    swap_mat[...] = jnp.where(hit, jnp.where(second, 1.0, -1.0), 0.0).astype(BF16)
    ones_mat[...] = jnp.where((row_id // HEAD) == (col_id // HEAD), 1.0, 0.0).astype(BF16)
    spread = jnp.where(
        row_id[:HEAD] == (col_id[:HEAD] & (HEAD - 1)), 1.0, 0.0
    ).astype(BF16)
    spread_swapped = jnp.where(
        row_id[:HEAD] == (partner_col[:HEAD] & (HEAD - 1)), 1.0, 0.0
    ).astype(BF16)
    lane_head = lax.broadcasted_iota(jnp.int32, (1, BLOCK), 1) // HEAD
    masks = [jnp.where(lane_head == p, 1.0, 0.0).astype(BF16) for p in range(GROUP)]

    pl.semaphore_wait(barrier, 1 + (here // 2) % 2 + (here // 4) % 2 + jnp.minimum(me, 1))

    for axis, (_, down, _, target) in enumerate(ways):
        @pl.when(down)
        def _(axis=axis, target=target):
            pl.semaphore_signal(above.at[axis], inc=1, device_id=target)

    part = k_ref.shape[1] // HALVES

    stores = (k_all, v_all)
    owns = (k_ref, v_ref)

    def kv_copy(way, step, kind, side):
        block = me - step if way == 0 else me + step
        target = me + 1 if way == 0 else me - 1
        columns = pl.ds(side * part, part)
        window = stores[kind].at[pl.ds(block * tokens, tokens), columns]
        return pltpu.make_async_remote_copy(
            src_ref=owns[kind].at[:, columns] if step == 0 else window,
            dst_ref=window,
            send_sem=kv_send.at[way, step, side, kind],
            recv_sem=kv_recv.at[way, step, side, kind],
            device_id={"sp": target},
        )

    def kv_sends(way, step):
        if way == 0:
            return jnp.logical_and(has_right, me - step >= 0)
        return jnp.logical_and(has_left, me + step < sp)

    def kv_start(way, step, kind, side):
        @pl.when(kv_sends(way, step))
        def _():
            kv_copy(way, step, kind, side).start()

    def kv_arrive(step, kind, side):
        for way in (0, 1):
            source = me - 1 - step if way == 0 else me + 1 + step
            arrives = source >= 0 if way == 0 else source < sp

            @pl.when(arrives)
            def _(way=way, source=source):
                window = stores[kind].at[
                    pl.ds(source * tokens, tokens), pl.ds(side * part, part)
                ]
                pltpu.make_async_remote_copy(
                    src_ref=window,
                    dst_ref=window,
                    send_sem=kv_send.at[way, step, side, kind],
                    recv_sem=kv_recv.at[way, step, side, kind],
                    device_id={"sp": me},
                ).wait_recv()

            if step + 1 < sp - 1:
                kv_start(way, step + 1, kind, side)


    odd = me % 2
    zmate = me + 1 - 2 * odd
    inner = (me + 1) // 2 % 2 == 1
    outer = jnp.logical_not(inner)
    shares = ((inner, 0, TO_END), (outer, half - TO_INNER, TO_INNER))
    mate_x, mate_y, mate_d = mate + flip_x, mate + flip_y, mate + flip_x + flip_y

    starts = [sum(CHUNKS[:j]) for j in range(len(CHUNKS))]
    pieces = {"own": (mate, 0, depth)}
    for j, (start, size) in enumerate(zip(starts, CHUNKS)):
        pieces["x", j] = (dev_x, half + start, size)
        pieces["y", j] = (dev_y, start, size)
        pieces["dx", j] = (dev_d, start, size)
        pieces["dy", j] = (dev_d, half + start, size)
    for name, shard, base in (("x", dev_x, 0), ("y", dev_y, half)):
        pieces[name, "middle"] = (shard, base + TO_END, half - TO_END - TO_INNER)
        for role, (_, start, size) in enumerate(shares):
            pieces[name, "share", role] = (shard, base + start, size)
    across = {"x": mate_x, "y": mate_y, "dx": mate_d, "dy": mate_d}
    for name in [name for name in pieces if name != "own"]:
        start, size = pieces[name][1:]
        pieces["mate", name] = (across[name[0]], start, size)
        if name[1] == "share":
            pieces["zed", name] = pieces[name]
    order = {name: i for i, name in enumerate(pieces)}
    sent = []

    def w_copy(name, shard, start, size, target, own=False):
        window = w_all.at[shard, pl.ds(start, size)]
        return pltpu.make_async_remote_copy(
            src_ref=w_ref.at[pl.ds(start, size)] if own else window,
            dst_ref=window,
            send_sem=w_send.at[order[name]],
            recv_sem=w_recv.at[order[name]],
            device_id=target,
        )

    def w_give(name, shard, start, size, target, own=False):
        copy = w_copy(name, shard, start, size, target, own)
        copy.start()
        sent.append((name, copy))

    def w_own(name, target):
        w_give(name, here, *pieces[name][1:], {"dp": target}, own=True)

    def w_wait(name):
        w_copy(name, *pieces[name], {"dp": mate}).wait_recv()

    def w_take(name):
        w_wait(name)
        piece = pieces[name]
        if name[1] in range(len(CHUNKS)):
            if name[0] == "x":
                w_give(("dy", name[1]), *piece, {"dp": dev_y})
            if name[0] == "y":
                w_give(("dx", name[1]), *piece, {"dp": dev_x})
        w_give(("mate", name), *piece, {"dp": mate})

    def w_share_own(name):
        for role, (chosen, _, _) in enumerate(shares):
            @pl.when(chosen)
            def _(key=(name, "share", role)):
                target = dev_x if name == "x" else dev_y
                w_copy(key, here, *pieces[key][1:], {"dp": target}, own=True).start()

    def w_share_near(role):
        @pl.when(shares[role][0])
        def _():
            for name in ("x", "y"):
                key = (name, "share", role)
                w_wait(key)
                w_copy(("zed", key), *pieces[key], {"sp": zmate}).start()
                w_copy(("mate", key), *pieces[key], {"dp": mate}).start()

    def w_share_far(role):
        @pl.when(shares[1 - role][0])
        def _():
            for name in ("x", "y"):
                key = (name, "share", role)
                w_wait(("zed", key))
                w_copy(("mate", key), *pieces[key], {"dp": mate}).start()

    def w_share_sent(name):
        for role, (chosen, _, _) in enumerate(shares):
            @pl.when(chosen)
            def _(key=(name, "share", role)):
                for form in (key, ("zed", key)):
                    w_copy(form, *pieces[key], {"dp": mate}).wait_send()

    def w_share_done(name):
        for role in range(len(shares)):
            key = (name, "share", role)
            w_copy(("mate", key), *pieces[key], {"dp": mate}).wait_send()

    def settle(names):
        for name, copy in [item for item in sent if item[0] in names]:
            copy.wait_send()
            sent.remove((name, copy))

    def own_list(name):
        return [(name, j) for j in range(len(CHUNKS))], (name, "middle")

    def w_start(name, target):
        chunks, middle = own_list(name)
        for key in chunks:
            w_copy(key, here, *pieces[key][1:], {"dp": target}, own=True).start()
        w_share_own(name)
        w_copy(middle, here, *pieces[middle][1:], {"dp": target}, own=True).start()

    def kv_begin(way):
        for kind in (0, 1):
            for side in range(HALVES):
                kv_copy(way, 0, kind, side).start()

    begins = (
        (lambda: w_start("x", dev_x),) * 2,
        (lambda: w_start("y", dev_y),) * 2,
        (lambda: kv_begin(0), lambda: kv_begin(1)),
    )
    for (_, down, _, _), (_, start) in zip(ways, begins):
        pl.when(down)(start)
    for name, target in (("x", dev_x), ("y", dev_y)):
        chunks, middle = own_list(name)
        for key in [*chunks, middle]:
            sent.append((key, w_copy(key, here, *pieces[key][1:], {"dp": target}, own=True)))
    w_own("own", mate)
    for axis, ((up, _, _, _), (start, _)) in enumerate(zip(ways, begins)):
        @pl.when(up)
        def _(axis=axis, start=start):
            pl.semaphore_wait(above.at[axis], 1)
            start()

    def turned(x, rows, which, scale):
        xf = x.astype(F32)
        square = xf * xf
        high = square.astype(BF16)
        low = (square - high.astype(F32)).astype(BF16)
        size = x.shape[1]
        ones = ones_mat[:size, :size]
        mean = (dot(high, ones) + dot(low, ones)) * (1.0 / HEAD)
        inverse = lax.rsqrt(mean + EPSILON) * scale
        swapped = dot(x, swap_mat[:size, :size])
        cosines = tables[0, rows, :]
        sines = tables[1, rows, :]
        if size > 2 * HEAD:
            cosines = jnp.concatenate([cosines, cosines], axis=1)
            sines = jnp.concatenate([sines, sines], axis=1)
        cosines = cosines * gains[2 * which, 0:1, :size]
        sines = sines * gains[2 * which + 1, 0:1, :size]
        return ((xf * cosines + swapped * sines) * inverse).astype(BF16)

    locals_[5].wait()
    locals_[6].wait()
    for i, gain_ref in enumerate((qg_ref, kg_ref)):
        gain = jnp.broadcast_to(gain_ref[...], (16, HEAD))
        first = gain.astype(BF16)
        rest = gain - first.astype(F32)
        mid = rest.astype(BF16)
        low = (rest - mid.astype(F32)).astype(BF16)
        for j, matrix in enumerate((spread, spread_swapped)):
            gains[2 * i + j] = (dot(first, matrix) + dot(mid, matrix)) + dot(low, matrix)

    locals_[3].wait()
    locals_[4].wait()
    locals_[7].wait()
    own_rows = pl.ds(pl.multiple_of(me * tokens, 64), tokens)
    for b in range(KVH):
        columns = slice(b * BLOCK, (b + 1) * BLOCK)
        query = turned(q_raw[:, columns], own_rows, 0, HEAD ** (-0.5))
        parts = [query[:WIDTH] * mask for mask in masks] + [query[WIDTH:] * mask for mask in masks]
        held = b % 2 * HEAD
        fold = jnp.where(row_id[:part] - held == (col_id[:part] & (HEAD - 1)), 1.0, 0.0)
        q_t[b] = cross(fold.astype(BF16), jnp.concatenate(parts, axis=0)).astype(BF16)

    eye = jnp.where(row_id == col_id, 1.0, 0.0).astype(BF16)
    far = 1 - me // 2
    blocks = [me, zmate, far + 1, 3 * far][:sp]
    spans = [pl.ds(pl.multiple_of(block * tokens, 64), tokens) for block in blocks]
    heads = KVH // HALVES
    rest = tokens - WIDTH
    final = sp - 1

    def score(turn, side):
        lanes = slice(side * part, (side + 1) * part)
        rows = spans[turn]
        key_side = turned(k_all[rows, lanes], rows, 1, 1.0)
        for b in range(side * heads, (side + 1) * heads):
            scores = dot(key_side, q_t[b])
            high = jnp.max(scores, axis=0, keepdims=True)
            if turn < final:
                weights = jnp.exp(scores - high)
                expo[turn, b] = weights
                peak[turn, b] = high
                total[turn, b] = jnp.sum(weights, axis=0, keepdims=True)
                continue
            for t in range(turn):
                high = jnp.maximum(high, peak[t, b])
            weights = jnp.exp(scores - high)
            norm = jnp.sum(weights, axis=0, keepdims=True)
            keeps = [jnp.exp(peak[t, b] - high) for t in range(turn)]
            for t in range(turn):
                norm = norm + total[t, b] * keeps[t]
            inverse = 1.0 / norm
            for t in range(turn):
                mixed[b, t * tokens : (t + 1) * tokens, :] = (
                    expo[t, b] * (keeps[t] * inverse)
                ).astype(BF16)
            mixed[b, turn * tokens :, :] = (weights * inverse).astype(BF16)

    def values(blocks, side):
        lanes = slice(side * part, (side + 1) * part)
        stack = jnp.concatenate([v_all[spans[t], lanes] for t in blocks], axis=0)
        result = cross(eye[:part, :part], stack).astype(BF16)
        if blocks[0] == final:
            v_last[lanes, :] = result
        else:
            v_turned[lanes, blocks[0] * tokens : (blocks[-1] + 1) * tokens] = result

    def each_head(side):
        for b in range(side * heads, (side + 1) * heads):
            yield b, slice(b * HEAD, (b + 1) * HEAD)

    def early(side):
        for b, value_rows in each_head(side):
            partial[b] = dot(v_turned[value_rows, :], mixed[b, : final * tokens, :])

    def gather(side):
        for b, value_rows in each_head(side):
            product = partial[b] + dot(v_last[value_rows, :], mixed[b, final * tokens :, :])
            for p in range(0, GROUP, 2):
                lanes = slice(b * BLOCK + p * HEAD, b * BLOCK + (p + 2) * HEAD)
                two = [product[:, i * WIDTH : (i + 1) * WIDTH] for i in (p, p + 1)]
                att[:WIDTH, lanes] = jnp.concatenate(two, axis=0).T.astype(BF16)
                start = GROUP * WIDTH + p * rest
                two = product[:, start : start + 2 * rest].T
                two = jnp.concatenate([two[:rest], two[rest:]], axis=1)
                att[WIDTH:, lanes] = two.astype(BF16)

    lots = len(CHUNKS)
    columns_each = w_ref.shape[1]
    late = LATE
    tails = {2: [0], 3: [half], 4: [0], 5: [half]}
    tails[6] = tails[7] = [half - late, depth - late]

    def columns_of(shard):
        return pl.ds(pl.multiple_of(shard * columns_each, columns_each), columns_each)

    def product(shard, start, size):
        rows = pl.ds(start, size)
        return dot(att[:, rows], w_all[shard, rows, :])

    def squares_of(result):
        square = result * result
        return sum(square[:, i : i + 128] for i in range(0, columns_each, 128))

    slots = [here, mate, dev_x, dev_y, mate_x, mate_y, dev_d, mate_d]

    def project(slot, squares):
        shard = slots[slot]
        result = dot(att[...], w_all[shard])
        proj[slot] = result * og_ref[:, columns_of(shard)]
        return squares + squares_of(result)

    def begin(slot):
        done, result = 0, 0.0
        for start in [*tails[slot], depth]:
            if start > done:
                result = result + product(slots[slot], done, start - done)
            done = start + late
        proj[slot] = result

    def end(slot):
        result = proj[slot]
        for start in tails[slot]:
            result = result + product(slots[slot], start, late)
        return result

    def end_early(slot, squares):
        result = end(slot)
        proj[slot] = result * og_ref[:, columns_of(slots[slot])]
        return squares + squares_of(result)

    def take(*names):
        for name in names:
            w_take(("x", name))
            w_take(("y", name))

    def take_far(j):
        w_take(("dx", j))
        w_take(("dy", j))

    locals_[0].wait()
    for side in range(HALVES):
        score(0, side)
    locals_[1].wait()

    jobs = {
        (0, 1, 0): lambda: take(0),
        (0, 1, 1): lambda: take(1),
        (1, 0, 0): lambda: take(*range(2, lots)),
        (1, 1, 0): lambda: w_share_near(1),
        (1, 1, 1): lambda: w_share_near(0),
        (2, 0, 0): lambda: take("middle"),
    }
    for step in range(sp - 1):
        turn = step + 1
        for kind in (0, 1):
            for side in range(HALVES):
                kv_arrive(step, kind, side)
                if kind == 0:
                    score(turn, side)
                    if turn == final:
                        if turn == 1:
                            values([0], side)
                        early(side)
                elif turn == final:
                    values([final], side)
                    gather(side)
                    if side == 0:
                        take_far(0)
                elif turn == 1:
                    values([0, 1], side)
                else:
                    values([turn], side)
                if (step, kind, side) in jobs:
                    jobs.pop((step, kind, side))()
    for job in jobs.values():
        job()

    w_share_far(1)
    locals_[2].wait()
    squares = project(0, jnp.zeros((tokens, 128), F32))
    w_wait("own")
    squares = project(1, squares)
    begin(2)
    begin(3)
    for j in range(1, lots - 1):
        take_far(j)
    for slot, name in ((4, "x"), (5, "y")):
        for piece in (*range(lots), "middle"):
            w_wait(("mate", (name, piece)))
        w_wait(("mate", (name, "share", 1)))
        begin(slot)
    begin(6)
    settle([name for name, _ in sent if not {"dx", "dy"} & {name[0], name[1][0] if name[0] == "mate" else ""}])
    for name in ("x", "y"):
        w_share_sent(name)
    for step in range(sp - 1):
        for way in (0, 1):
            @pl.when(kv_sends(way, step))
            def _(way=way, step=step):
                for kind in (0, 1):
                    for side in range(HALVES):
                        kv_copy(way, step, kind, side).wait_send()
    w_share_far(0)
    take_far(lots - 1)
    for slot in (2, 3):
        squares = end_early(slot, squares)
    for j in range(lots - 1):
        w_wait(("mate", ("dx", j)))
        w_wait(("mate", ("dy", j)))
    begin(7)
    for slot, name in ((4, "x"), (5, "y")):
        w_wait(("mate", (name, "share", 0)))
        squares = end_early(slot, squares)
    for axis in ("dx", "dy"):
        w_wait(("mate", (axis, lots - 1)))
    ends = [end(6), end(7)]
    for result in ends:
        squares = squares + squares_of(result)
    squares = jnp.sum(squares, axis=1, keepdims=True)
    inverse = lax.rsqrt(squares * (1.0 / (columns_each * dp)) + EPSILON)
    for slot, shard in enumerate(slots):
        columns = columns_of(shard)
        if slot < 6:
            result = proj[slot]
        else:
            result = ends[slot - 6] * og_ref[:, columns]
        out_ref[:, columns] = (result * inverse).astype(BF16)

    settle([name for name, _ in sent])
    for name in ("x", "y"):
        w_share_done(name)


def per_device_fused(sp, dp, queries, keys, values, query_gain, key_gain, out_weight, out_gain):
    tokens = queries.shape[1]
    depth, columns = out_weight.shape
    hidden = queries.shape[2]
    kv_width = keys.shape[2]
    seq_len = tokens * sp
    hbm_spec = pl.BlockSpec(memory_space=pltpu.HBM)
    vmem_spec = pl.BlockSpec(memory_space=pltpu.VMEM)
    result = pl.pallas_call(
        functools.partial(kernel, sp, dp),
        out_shape=pltpu.VMEM((tokens, columns * dp), BF16),
        in_specs=[hbm_spec] * 8,
        out_specs=vmem_spec,
        scratch_shapes=[
            pltpu.VMEM((tokens, hidden), BF16),
            pltpu.VMEM((seq_len, kv_width), BF16),
            pltpu.VMEM((seq_len, kv_width), BF16),
            pltpu.VMEM((2, seq_len, 2 * HEAD), F32),
            pltpu.VMEM((dp, depth, columns), BF16),
            pltpu.VMEM((4, 16, BLOCK), F32),
            pltpu.VMEM((BLOCK, BLOCK), BF16),
            pltpu.VMEM((BLOCK, BLOCK), BF16),
            pltpu.VMEM((KVH, kv_width // HALVES, GROUP * tokens), BF16),
            pltpu.VMEM((kv_width, seq_len - tokens), BF16),
            pltpu.VMEM((kv_width, tokens), BF16),
            pltpu.VMEM((KVH, HEAD, GROUP * tokens), F32),
            pltpu.VMEM((sp - 1, KVH, tokens, GROUP * tokens), F32),
            pltpu.VMEM((sp - 1, KVH, 1, GROUP * tokens), F32),
            pltpu.VMEM((sp - 1, KVH, 1, GROUP * tokens), F32),
            pltpu.VMEM((KVH, seq_len, GROUP * tokens), BF16),
            pltpu.VMEM((tokens, hidden), BF16),
            pltpu.VMEM((dp, tokens, columns), F32),
            pltpu.VMEM((1, HEAD), F32),
            pltpu.VMEM((1, HEAD), F32),
            pltpu.VMEM((1, columns * dp), F32),
            pltpu.SemaphoreType.REGULAR((3,)),
            pltpu.SemaphoreType.DMA((8,)),
            pltpu.SemaphoreType.DMA((2, sp - 1, HALVES, 2)),
            pltpu.SemaphoreType.DMA((2, sp - 1, HALVES, 2)),
            pltpu.SemaphoreType.DMA((PIECES,)),
            pltpu.SemaphoreType.DMA((PIECES,)),
        ],
        compiler_params=pltpu.CompilerParams(
            collective_id=0, has_side_effects=True, vmem_limit_bytes=66000000
        ),
    )(
        queries[0], keys[0], values[0], query_gain[None], key_gain[None],
        out_weight, out_gain[None], jnp.asarray(position_tables(seq_len)),
    )
    return result[None]


def solution(mesh):
    sp, dp = mesh.shape["sp"], mesh.shape["dp"]
    if dp == 8 and sp >= 2 and sp % 2 == 0 and sp <= 4:
        body = functools.partial(per_device_fused, sp, dp)
    else:
        body = per_device_general
    return jax.shard_map(
        body,
        mesh=mesh,
        in_specs=(
            P("dp", "sp", None),
            P("dp", "sp", None),
            P("dp", "sp", None),
            P(),
            P(),
            P(None, "dp"),
            P(),
        ),
        out_specs=P("dp", "sp", None),
        check_vma=False,
    )
```

```python
import functools

import jax
import jax.numpy as jnp
import numpy as np
from jax import lax
from jax.experimental import pallas as pl
from jax.experimental.pallas import tpu as pltpu
from jax.sharding import PartitionSpec as P

QH = 16
KVH = 4
HEAD = 64
GRID_W = 64
GROUP = QH // KVH
HALVES = 2
BLOCK = GROUP * HEAD
WIDTH = 128

TO_END = 128
TO_INNER = 192
CHUNKS = (256, 128, 128)
LATE = 128
PIECES = 8 * len(CHUNKS) + 17


EPSILON = 1e-06
ROTARY_BASE = 10000.0

F32 = jnp.float32
BF16 = jnp.bfloat16


def rotate(vectors, positions, width):
    half_width = width // 2
    frequency = ROTARY_BASE ** (-jnp.arange(0, width, 2, dtype=jnp.float32) / width)
    angles = positions.astype(jnp.float32)[:, None] * frequency[None, :]
    cosines = jnp.cos(angles)[:, None, :]
    sine_table = jnp.sin(angles)[:, None, :]
    first_half = vectors[..., :half_width]
    second_half = vectors[..., half_width:]
    return jnp.concatenate(
        [
            first_half * cosines - second_half * sine_table,
            second_half * cosines + first_half * sine_table,
        ],
        axis=-1,
    )


def prepare(vectors, gain_vector, grid_row, grid_col):
    vectors = vectors.astype(jnp.float32)
    vectors = (
        vectors
        * lax.rsqrt(jnp.mean(vectors * vectors, axis=-1, keepdims=True) + EPSILON)
        * gain_vector
    )
    half_width = HEAD // 2
    turned = jnp.concatenate(
        [
            rotate(vectors[..., :half_width], grid_row, half_width),
            rotate(vectors[..., half_width:], grid_col, half_width),
        ],
        axis=-1,
    )
    return turned.astype(jnp.bfloat16)


def softmax_rows(scores):
    row_max = jnp.max(scores, axis=-1, keepdims=True)
    exponent = jnp.exp(scores - row_max)
    return exponent / jnp.sum(exponent, axis=-1, keepdims=True)


def per_device_general(queries, keys, values, query_gain, key_gain, out_weight, out_gain):
    sp_count = lax.axis_size("sp")
    tokens_here = queries.shape[1]
    seq_len = tokens_here * sp_count
    score_scale = HEAD ** (-0.5)
    offset = lax.axis_index("sp") * tokens_here
    positions = offset + jnp.arange(tokens_here, dtype=jnp.int32)
    grid_row = positions // GRID_W
    grid_col = positions % GRID_W
    query_rot = prepare(queries[0].reshape(tokens_here, QH, HEAD), query_gain, grid_row, grid_col)
    key_rot = prepare(keys[0].reshape(tokens_here, KVH, HEAD), key_gain, grid_row, grid_col)
    value_heads = values[0].reshape(tokens_here, KVH, HEAD)
    kv_pairs = jnp.concatenate([key_rot, value_heads], axis=2)
    all_pairs = lax.all_gather(
        kv_pairs.reshape(tokens_here, KVH * 2 * HEAD), "sp", axis=0, tiled=True
    )
    all_pairs = all_pairs.reshape(seq_len, KVH, 2, HEAD)
    key_all = all_pairs[:, :, 0].transpose(1, 0, 2)
    value_all = all_pairs[:, :, 1].transpose(1, 0, 2)
    query_groups = query_rot.reshape(tokens_here, KVH, QH // KVH, HEAD).transpose(1, 0, 2, 3)

    def attend_group(operands):
        query_group, key_head, value_head = operands
        scores = (
            jnp.einsum("qgd,kd->gqk", query_group, key_head, preferred_element_type=jnp.float32)
            * score_scale
        )
        attn_weights = softmax_rows(scores).astype(jnp.bfloat16)
        return jnp.einsum(
            "gqk,kd->qgd", attn_weights, value_head, preferred_element_type=jnp.float32
        ).astype(jnp.bfloat16)

    results = lax.map(attend_group, (query_groups, key_all, value_all))
    attended = results.transpose(1, 0, 2, 3).reshape(tokens_here, QH * HEAD)
    projected = jnp.dot(
        attended,
        lax.all_gather(out_weight, "dp", axis=1, tiled=True),
        preferred_element_type=jnp.float32,
    )
    normed = (
        projected
        * lax.rsqrt(jnp.mean(projected * projected, axis=-1, keepdims=True) + EPSILON)
        * out_gain
    )
    return normed.astype(jnp.bfloat16)[None]


def position_tables(seq_len):
    width = HEAD // 2
    frequency = np.float32(ROTARY_BASE) ** (
        -np.arange(0, width, 2, dtype=np.float32) / np.float32(width)
    )
    position = np.arange(seq_len)
    parts = []
    for coordinate in (position // GRID_W, position % GRID_W):
        angles = coordinate.astype(np.float32)[:, None] * frequency[None, :]
        parts += [angles, angles]
    angles = np.concatenate(parts * 2, axis=1).astype(np.float64)
    return np.stack([np.cos(angles), np.sin(angles)]).astype(np.float32)


def dot(a, b):
    return jnp.dot(a, b, preferred_element_type=F32)


def cross(a, b):
    return lax.dot_general(a, b, (((1,), (1,)), ((), ())), preferred_element_type=F32)


def kernel(
    sp, dp,
    q_ref, k_ref, v_ref, qg_hbm, kg_hbm, w_ref, og_hbm, table_ref,
    out_ref,
    q_raw, k_all, v_all, tables, w_all, gains,
    swap_mat, ones_mat, q_t, v_turned, v_last, partial,
    expo, peak, total, mixed, att, proj,
    qg_ref, kg_ref, og_ref, above, local_sem, kv_send, kv_recv, w_send, w_recv,
):
    tokens = q_raw.shape[0]
    depth = w_ref.shape[0]
    half = depth // 2
    me = lax.axis_index("sp")
    here = lax.axis_index("dp")
    mate = here + 1 - 2 * (here % 2)
    flip_x = 2 - 4 * ((here // 2) % 2)
    flip_y = 4 - 8 * ((here // 4) % 2)
    dev_x = here + flip_x
    dev_y = here + flip_y
    dev_d = here + flip_x + flip_y

    barrier = pltpu.get_barrier_semaphore()
    has_left = me > 0
    has_right = me < sp - 1

    low_x, low_y = (here // 2) % 2 == 0, (here // 4) % 2 == 0
    high_x, high_y = jnp.logical_not(low_x), jnp.logical_not(low_y)
    ways = (
        (low_x, high_x, {"dp": dev_x}, {"dp": dev_x}),
        (low_y, high_y, {"dp": dev_y}, {"dp": dev_y}),
        (has_right, has_left, {"sp": me + 1}, {"sp": me - 1}),
    )

    pl.semaphore_signal(barrier, inc=1, device_id={"dp": mate})
    for up, _, target, _ in ways:
        @pl.when(up)
        def _(target=target):
            pl.semaphore_signal(barrier, inc=1, device_id=target)

    locals_ = [
        pltpu.make_async_copy(k_ref, k_all.at[pl.ds(me * tokens, tokens)], local_sem.at[0]),
        pltpu.make_async_copy(v_ref, v_all.at[pl.ds(me * tokens, tokens)], local_sem.at[1]),
        pltpu.make_async_copy(w_ref, w_all.at[here], local_sem.at[2]),
        pltpu.make_async_copy(q_ref, q_raw, local_sem.at[3]),
        pltpu.make_async_copy(table_ref, tables, local_sem.at[4]),
        pltpu.make_async_copy(qg_hbm, qg_ref, local_sem.at[5]),
        pltpu.make_async_copy(kg_hbm, kg_ref, local_sem.at[6]),
        pltpu.make_async_copy(og_hbm, og_ref, local_sem.at[7]),
    ]
    for copy in locals_:
        copy.start()

    row_id = lax.broadcasted_iota(jnp.int32, (BLOCK, BLOCK), 0)
    col_id = lax.broadcasted_iota(jnp.int32, (BLOCK, BLOCK), 1)
    quarter = HEAD // 4
    second = (col_id & (HEAD // 2 - 1)) >= quarter
    partner_col = jnp.where(second, col_id - quarter, col_id + quarter)
    hit = row_id == partner_col
    swap_mat[...] = jnp.where(hit, jnp.where(second, 1.0, -1.0), 0.0).astype(BF16)
    ones_mat[...] = jnp.where((row_id // HEAD) == (col_id // HEAD), 1.0, 0.0).astype(BF16)
    spread = jnp.where(
        row_id[:HEAD] == (col_id[:HEAD] & (HEAD - 1)), 1.0, 0.0
    ).astype(BF16)
    spread_swapped = jnp.where(
        row_id[:HEAD] == (partner_col[:HEAD] & (HEAD - 1)), 1.0, 0.0
    ).astype(BF16)
    lane_head = lax.broadcasted_iota(jnp.int32, (1, BLOCK), 1) // HEAD
    masks = [jnp.where(lane_head == p, 1.0, 0.0).astype(BF16) for p in range(GROUP)]

    pl.semaphore_wait(barrier, 1 + (here // 2) % 2 + (here // 4) % 2 + jnp.minimum(me, 1))

    for axis, (_, down, _, target) in enumerate(ways):
        @pl.when(down)
        def _(axis=axis, target=target):
            pl.semaphore_signal(above.at[axis], inc=1, device_id=target)

    part = k_ref.shape[1] // HALVES

    stores = (k_all, v_all)
    owns = (k_ref, v_ref)

    def kv_copy(way, step, kind, side):
        block = me - step if way == 0 else me + step
        target = me + 1 if way == 0 else me - 1
        columns = pl.ds(side * part, part)
        window = stores[kind].at[pl.ds(block * tokens, tokens), columns]
        return pltpu.make_async_remote_copy(
            src_ref=owns[kind].at[:, columns] if step == 0 else window,
            dst_ref=window,
            send_sem=kv_send.at[way, step, side, kind],
            recv_sem=kv_recv.at[way, step, side, kind],
            device_id={"sp": target},
        )

    def kv_sends(way, step):
        if way == 0:
            return jnp.logical_and(has_right, me - step >= 0)
        return jnp.logical_and(has_left, me + step < sp)

    def kv_start(way, step, kind, side):
        @pl.when(kv_sends(way, step))
        def _():
            kv_copy(way, step, kind, side).start()

    def kv_arrive(step, kind, side):
        for way in (0, 1):
            source = me - 1 - step if way == 0 else me + 1 + step
            arrives = source >= 0 if way == 0 else source < sp

            @pl.when(arrives)
            def _(way=way, source=source):
                window = stores[kind].at[
                    pl.ds(source * tokens, tokens), pl.ds(side * part, part)
                ]
                pltpu.make_async_remote_copy(
                    src_ref=window,
                    dst_ref=window,
                    send_sem=kv_send.at[way, step, side, kind],
                    recv_sem=kv_recv.at[way, step, side, kind],
                    device_id={"sp": me},
                ).wait_recv()

            if step + 1 < sp - 1:
                kv_start(way, step + 1, kind, side)


    odd = me % 2
    zmate = me + 1 - 2 * odd
    inner = (me + 1) // 2 % 2 == 1
    outer = jnp.logical_not(inner)
    shares = ((inner, 0, TO_END), (outer, half - TO_INNER, TO_INNER))
    mate_x, mate_y, mate_d = mate + flip_x, mate + flip_y, mate + flip_x + flip_y

    starts = [sum(CHUNKS[:j]) for j in range(len(CHUNKS))]
    pieces = {"own": (mate, 0, depth)}
    for j, (start, size) in enumerate(zip(starts, CHUNKS)):
        pieces["x", j] = (dev_x, half + start, size)
        pieces["y", j] = (dev_y, start, size)
        pieces["dx", j] = (dev_d, start, size)
        pieces["dy", j] = (dev_d, half + start, size)
    for name, shard, base in (("x", dev_x, 0), ("y", dev_y, half)):
        pieces[name, "middle"] = (shard, base + TO_END, half - TO_END - TO_INNER)
        for role, (_, start, size) in enumerate(shares):
            pieces[name, "share", role] = (shard, base + start, size)
    across = {"x": mate_x, "y": mate_y, "dx": mate_d, "dy": mate_d}
    for name in [name for name in pieces if name != "own"]:
        start, size = pieces[name][1:]
        pieces["mate", name] = (across[name[0]], start, size)
        if name[1] == "share":
            pieces["zed", name] = pieces[name]
    order = {name: i for i, name in enumerate(pieces)}
    sent = []

    def w_copy(name, shard, start, size, target, own=False):
        window = w_all.at[shard, pl.ds(start, size)]
        return pltpu.make_async_remote_copy(
            src_ref=w_ref.at[pl.ds(start, size)] if own else window,
            dst_ref=window,
            send_sem=w_send.at[order[name]],
            recv_sem=w_recv.at[order[name]],
            device_id=target,
        )

    def w_give(name, shard, start, size, target, own=False):
        copy = w_copy(name, shard, start, size, target, own)
        copy.start()
        sent.append((name, copy))

    def w_own(name, target):
        w_give(name, here, *pieces[name][1:], {"dp": target}, own=True)

    def w_wait(name):
        w_copy(name, *pieces[name], {"dp": mate}).wait_recv()

    def w_take(name):
        w_wait(name)
        piece = pieces[name]
        if name[1] in range(len(CHUNKS)):
            if name[0] == "x":
                w_give(("dy", name[1]), *piece, {"dp": dev_y})
            if name[0] == "y":
                w_give(("dx", name[1]), *piece, {"dp": dev_x})
        w_give(("mate", name), *piece, {"dp": mate})

    def w_share_own(name):
        for role, (chosen, _, _) in enumerate(shares):
            @pl.when(chosen)
            def _(key=(name, "share", role)):
                target = dev_x if name == "x" else dev_y
                w_copy(key, here, *pieces[key][1:], {"dp": target}, own=True).start()

    def w_share_near(role):
        @pl.when(shares[role][0])
        def _():
            for name in ("x", "y"):
                key = (name, "share", role)
                w_wait(key)
                w_copy(("zed", key), *pieces[key], {"sp": zmate}).start()
                w_copy(("mate", key), *pieces[key], {"dp": mate}).start()

    def w_share_far(role):
        @pl.when(shares[1 - role][0])
        def _():
            for name in ("x", "y"):
                key = (name, "share", role)
                w_wait(("zed", key))
                w_copy(("mate", key), *pieces[key], {"dp": mate}).start()

    def w_share_sent(name):
        for role, (chosen, _, _) in enumerate(shares):
            @pl.when(chosen)
            def _(key=(name, "share", role)):
                for form in (key, ("zed", key)):
                    w_copy(form, *pieces[key], {"dp": mate}).wait_send()

    def w_share_done(name):
        for role in range(len(shares)):
            key = (name, "share", role)
            w_copy(("mate", key), *pieces[key], {"dp": mate}).wait_send()

    def settle(names):
        for name, copy in [item for item in sent if item[0] in names]:
            copy.wait_send()
            sent.remove((name, copy))

    def own_list(name):
        return [(name, j) for j in range(len(CHUNKS))], (name, "middle")

    def w_start(name, target):
        chunks, middle = own_list(name)
        for key in chunks:
            w_copy(key, here, *pieces[key][1:], {"dp": target}, own=True).start()
        w_share_own(name)
        w_copy(middle, here, *pieces[middle][1:], {"dp": target}, own=True).start()

    def kv_begin(way):
        for kind in (0, 1):
            for side in range(HALVES):
                kv_copy(way, 0, kind, side).start()

    begins = (
        (lambda: w_start("x", dev_x),) * 2,
        (lambda: w_start("y", dev_y),) * 2,
        (lambda: kv_begin(0), lambda: kv_begin(1)),
    )
    for (_, down, _, _), (_, start) in zip(ways, begins):
        pl.when(down)(start)
    for name, target in (("x", dev_x), ("y", dev_y)):
        chunks, middle = own_list(name)
        for key in [*chunks, middle]:
            sent.append((key, w_copy(key, here, *pieces[key][1:], {"dp": target}, own=True)))
    w_own("own", mate)
    for axis, ((up, _, _, _), (start, _)) in enumerate(zip(ways, begins)):
        @pl.when(up)
        def _(axis=axis, start=start):
            pl.semaphore_wait(above.at[axis], 1)
            start()

    def turned(x, rows, which, scale):
        xf = x.astype(F32)
        square = xf * xf
        high = square.astype(BF16)
        low = (square - high.astype(F32)).astype(BF16)
        size = x.shape[1]
        ones = ones_mat[:size, :size]
        mean = (dot(high, ones) + dot(low, ones)) * (1.0 / HEAD)
        inverse = lax.rsqrt(mean + EPSILON) * scale
        swapped = dot(x, swap_mat[:size, :size])
        cosines = tables[0, rows, :]
        sines = tables[1, rows, :]
        if size > 2 * HEAD:
            cosines = jnp.concatenate([cosines, cosines], axis=1)
            sines = jnp.concatenate([sines, sines], axis=1)
        cosines = cosines * gains[2 * which, 0:1, :size]
        sines = sines * gains[2 * which + 1, 0:1, :size]
        return ((xf * cosines + swapped * sines) * inverse).astype(BF16)

    locals_[5].wait()
    locals_[6].wait()
    for i, gain_ref in enumerate((qg_ref, kg_ref)):
        gain = jnp.broadcast_to(gain_ref[...], (16, HEAD))
        first = gain.astype(BF16)
        rest = gain - first.astype(F32)
        mid = rest.astype(BF16)
        low = (rest - mid.astype(F32)).astype(BF16)
        for j, matrix in enumerate((spread, spread_swapped)):
            gains[2 * i + j] = (dot(first, matrix) + dot(mid, matrix)) + dot(low, matrix)

    locals_[3].wait()
    locals_[4].wait()
    locals_[7].wait()
    own_rows = pl.ds(pl.multiple_of(me * tokens, 64), tokens)
    for b in range(KVH):
        columns = slice(b * BLOCK, (b + 1) * BLOCK)
        query = turned(q_raw[:, columns], own_rows, 0, HEAD ** (-0.5))
        parts = [query[:WIDTH] * mask for mask in masks] + [query[WIDTH:] * mask for mask in masks]
        held = b % 2 * HEAD
        fold = jnp.where(row_id[:part] - held == (col_id[:part] & (HEAD - 1)), 1.0, 0.0)
        q_t[b] = cross(fold.astype(BF16), jnp.concatenate(parts, axis=0)).astype(BF16)

    eye = jnp.where(row_id == col_id, 1.0, 0.0).astype(BF16)
    far = 1 - me // 2
    blocks = [me, zmate, far + 1, 3 * far][:sp]
    spans = [pl.ds(pl.multiple_of(block * tokens, 64), tokens) for block in blocks]
    heads = KVH // HALVES
    rest = tokens - WIDTH
    final = sp - 1

    def score(turn, side):
        lanes = slice(side * part, (side + 1) * part)
        rows = spans[turn]
        key_side = turned(k_all[rows, lanes], rows, 1, 1.0)
        for b in range(side * heads, (side + 1) * heads):
            scores = dot(key_side, q_t[b])
            high = jnp.max(scores, axis=0, keepdims=True)
            if turn < final:
                weights = jnp.exp(scores - high)
                expo[turn, b] = weights
                peak[turn, b] = high
                total[turn, b] = jnp.sum(weights, axis=0, keepdims=True)
                continue
            for t in range(turn):
                high = jnp.maximum(high, peak[t, b])
            weights = jnp.exp(scores - high)
            norm = jnp.sum(weights, axis=0, keepdims=True)
            keeps = [jnp.exp(peak[t, b] - high) for t in range(turn)]
            for t in range(turn):
                norm = norm + total[t, b] * keeps[t]
            inverse = 1.0 / norm
            for t in range(turn):
                mixed[b, t * tokens : (t + 1) * tokens, :] = (
                    expo[t, b] * (keeps[t] * inverse)
                ).astype(BF16)
            mixed[b, turn * tokens :, :] = (weights * inverse).astype(BF16)

    def values(blocks, side):
        lanes = slice(side * part, (side + 1) * part)
        stack = jnp.concatenate([v_all[spans[t], lanes] for t in blocks], axis=0)
        result = cross(eye[:part, :part], stack).astype(BF16)
        if blocks[0] == final:
            v_last[lanes, :] = result
        else:
            v_turned[lanes, blocks[0] * tokens : (blocks[-1] + 1) * tokens] = result

    def each_head(side):
        for b in range(side * heads, (side + 1) * heads):
            yield b, slice(b * HEAD, (b + 1) * HEAD)

    def early(side):
        for b, value_rows in each_head(side):
            partial[b] = dot(v_turned[value_rows, :], mixed[b, : final * tokens, :])

    def gather(side):
        for b, value_rows in each_head(side):
            product = partial[b] + dot(v_last[value_rows, :], mixed[b, final * tokens :, :])
            for p in range(0, GROUP, 2):
                lanes = slice(b * BLOCK + p * HEAD, b * BLOCK + (p + 2) * HEAD)
                two = [product[:, i * WIDTH : (i + 1) * WIDTH] for i in (p, p + 1)]
                att[:WIDTH, lanes] = jnp.concatenate(two, axis=0).T.astype(BF16)
                start = GROUP * WIDTH + p * rest
                two = product[:, start : start + 2 * rest].T
                two = jnp.concatenate([two[:rest], two[rest:]], axis=1)
                att[WIDTH:, lanes] = two.astype(BF16)

    lots = len(CHUNKS)
    columns_each = w_ref.shape[1]
    late = LATE
    tails = {2: [0], 3: [half], 4: [0], 5: [half]}
    tails[6] = tails[7] = [half - late, depth - late]

    def columns_of(shard):
        return pl.ds(pl.multiple_of(shard * columns_each, columns_each), columns_each)

    def product(shard, start, size):
        rows = pl.ds(start, size)
        return dot(att[:, rows], w_all[shard, rows, :])

    def squares_of(result):
        square = result * result
        return sum(square[:, i : i + 128] for i in range(0, columns_each, 128))

    slots = [here, mate, dev_x, dev_y, mate_x, mate_y, dev_d, mate_d]

    def project(slot, squares):
        shard = slots[slot]
        result = dot(att[...], w_all[shard])
        proj[slot] = result * og_ref[:, columns_of(shard)]
        return squares + squares_of(result)

    def begin(slot):
        done, result = 0, 0.0
        for start in [*tails[slot], depth]:
            if start > done:
                result = result + product(slots[slot], done, start - done)
            done = start + late
        proj[slot] = result

    def end(slot):
        result = proj[slot]
        for start in tails[slot]:
            result = result + product(slots[slot], start, late)
        return result

    def end_early(slot, squares):
        result = end(slot)
        proj[slot] = result * og_ref[:, columns_of(slots[slot])]
        return squares + squares_of(result)

    def take(*names):
        for name in names:
            w_take(("x", name))
            w_take(("y", name))

    def take_far(j):
        w_take(("dx", j))
        w_take(("dy", j))

    locals_[0].wait()
    for side in range(HALVES):
        score(0, side)
    locals_[1].wait()

    jobs = {
        (0, 1, 0): lambda: take(0),
        (0, 1, 1): lambda: take(1),
        (1, 0, 0): lambda: take(*range(2, lots)),
        (1, 1, 0): lambda: w_share_near(1),
        (1, 1, 1): lambda: w_share_near(0),
        (2, 0, 0): lambda: take("middle"),
    }
    for step in range(sp - 1):
        turn = step + 1
        for kind in (0, 1):
            for side in range(HALVES):
                kv_arrive(step, kind, side)
                if kind == 0:
                    score(turn, side)
                    if turn == final:
                        if turn == 1:
                            values([0], side)
                        early(side)
                elif turn == final:
                    values([final], side)
                    gather(side)
                elif turn == 1:
                    values([0, 1], side)
                else:
                    values([turn], side)
                if (step, kind, side) in jobs:
                    jobs.pop((step, kind, side))()
    for job in jobs.values():
        job()

    take_far(0)
    w_share_far(1)
    locals_[2].wait()
    squares = project(0, jnp.zeros((tokens, 128), F32))
    w_wait("own")
    squares = project(1, squares)
    begin(2)
    begin(3)
    for j in range(1, lots - 1):
        take_far(j)
    for slot, name in ((4, "x"), (5, "y")):
        for piece in (*range(lots), "middle"):
            w_wait(("mate", (name, piece)))
        w_wait(("mate", (name, "share", 1)))
        begin(slot)
    begin(6)
    settle([name for name, _ in sent if not {"dx", "dy"} & {name[0], name[1][0] if name[0] == "mate" else ""}])
    for name in ("x", "y"):
        w_share_sent(name)
    for step in range(sp - 1):
        for way in (0, 1):
            @pl.when(kv_sends(way, step))
            def _(way=way, step=step):
                for kind in (0, 1):
                    for side in range(HALVES):
                        kv_copy(way, step, kind, side).wait_send()
    w_share_far(0)
    take_far(lots - 1)
    for slot in (2, 3):
        squares = end_early(slot, squares)
    for j in range(lots - 1):
        w_wait(("mate", ("dx", j)))
        w_wait(("mate", ("dy", j)))
    begin(7)
    for slot, name in ((4, "x"), (5, "y")):
        w_wait(("mate", (name, "share", 0)))
        squares = end_early(slot, squares)
    for axis in ("dx", "dy"):
        w_wait(("mate", (axis, lots - 1)))
    ends = [end(6), end(7)]
    for result in ends:
        squares = squares + squares_of(result)
    squares = jnp.sum(squares, axis=1, keepdims=True)
    inverse = lax.rsqrt(squares * (1.0 / (columns_each * dp)) + EPSILON)
    for slot, shard in enumerate(slots):
        columns = columns_of(shard)
        if slot < 6:
            result = proj[slot]
        else:
            result = ends[slot - 6] * og_ref[:, columns]
        out_ref[:, columns] = (result * inverse).astype(BF16)

    settle([name for name, _ in sent])
    for name in ("x", "y"):
        w_share_done(name)


def per_device_fused(sp, dp, queries, keys, values, query_gain, key_gain, out_weight, out_gain):
    tokens = queries.shape[1]
    depth, columns = out_weight.shape
    hidden = queries.shape[2]
    kv_width = keys.shape[2]
    seq_len = tokens * sp
    hbm_spec = pl.BlockSpec(memory_space=pltpu.HBM)
    vmem_spec = pl.BlockSpec(memory_space=pltpu.VMEM)
    result = pl.pallas_call(
        functools.partial(kernel, sp, dp),
        out_shape=pltpu.VMEM((tokens, columns * dp), BF16),
        in_specs=[hbm_spec] * 8,
        out_specs=vmem_spec,
        scratch_shapes=[
            pltpu.VMEM((tokens, hidden), BF16),
            pltpu.VMEM((seq_len, kv_width), BF16),
            pltpu.VMEM((seq_len, kv_width), BF16),
            pltpu.VMEM((2, seq_len, 2 * HEAD), F32),
            pltpu.VMEM((dp, depth, columns), BF16),
            pltpu.VMEM((4, 16, BLOCK), F32),
            pltpu.VMEM((BLOCK, BLOCK), BF16),
            pltpu.VMEM((BLOCK, BLOCK), BF16),
            pltpu.VMEM((KVH, kv_width // HALVES, GROUP * tokens), BF16),
            pltpu.VMEM((kv_width, seq_len - tokens), BF16),
            pltpu.VMEM((kv_width, tokens), BF16),
            pltpu.VMEM((KVH, HEAD, GROUP * tokens), F32),
            pltpu.VMEM((sp - 1, KVH, tokens, GROUP * tokens), F32),
            pltpu.VMEM((sp - 1, KVH, 1, GROUP * tokens), F32),
            pltpu.VMEM((sp - 1, KVH, 1, GROUP * tokens), F32),
            pltpu.VMEM((KVH, seq_len, GROUP * tokens), BF16),
            pltpu.VMEM((tokens, hidden), BF16),
            pltpu.VMEM((dp, tokens, columns), F32),
            pltpu.VMEM((1, HEAD), F32),
            pltpu.VMEM((1, HEAD), F32),
            pltpu.VMEM((1, columns * dp), F32),
            pltpu.SemaphoreType.REGULAR((3,)),
            pltpu.SemaphoreType.DMA((8,)),
            pltpu.SemaphoreType.DMA((2, sp - 1, HALVES, 2)),
            pltpu.SemaphoreType.DMA((2, sp - 1, HALVES, 2)),
            pltpu.SemaphoreType.DMA((PIECES,)),
            pltpu.SemaphoreType.DMA((PIECES,)),
        ],
        compiler_params=pltpu.CompilerParams(
            collective_id=0, has_side_effects=True, vmem_limit_bytes=66000000
        ),
    )(
        queries[0], keys[0], values[0], query_gain[None], key_gain[None],
        out_weight, out_gain[None], jnp.asarray(position_tables(seq_len)),
    )
    return result[None]


def solution(mesh):
    sp, dp = mesh.shape["sp"], mesh.shape["dp"]
    if dp == 8 and sp >= 2 and sp % 2 == 0 and sp <= 4:
        body = functools.partial(per_device_fused, sp, dp)
    else:
        body = per_device_general
    return jax.shard_map(
        body,
        mesh=mesh,
        in_specs=(
            P("dp", "sp", None),
            P("dp", "sp", None),
            P("dp", "sp", None),
            P(),
            P(),
            P(None, "dp"),
            P(),
        ),
        out_specs=P("dp", "sp", None),
        check_vma=False,
    )
```
